128 devices in a mesh: sp: 64 (over z, y, x), tp: 2 (over core).
Axes of the slice: x: 4, y: 4, z: 4, core: 2. Of those that a mesh axis runs over, the one named last changes fastest.
Arguments:
- wide_inputs: bfloat16 [8192, 512], P('sp', 'tp'), may hold values from -6 to 6
- narrow_inputs: bfloat16 [8192, 512], P('sp', 'tp'), may hold values from -6 to 6
- wide_poles: float32 [2, 2, 32, 64], P(None, None, 'tp'), may hold values from -3.1416 to 3.1416, as said below
- narrow_poles: float32 [2, 2, 32, 32], P(None, None, 'tp'), may hold values from -3.1416 to 3.1416, as said below
- step_sizes: float32 [2, 2, 32], P(None, None, 'tp'), may hold values from 0 to 1, as said below
- forget: float32 [2, 2, 32, 8192], P(None, None, 'tp', 'sp'), may hold values from 0 to 2.2
- wide_in_map: float32 [2, 2, 32, 16, 64], P(None, None, 'tp'), may hold values from -2.5 to 2.5
- narrow_in_map: float32 [2, 2, 32, 16, 32], P(None, None, 'tp'), may hold values from -2.5 to 2.5
- wide_out_map: float32 [2, 2, 32, 16, 64], P(None, None, 'tp'), may hold values from -1.25 to 1.25
- narrow_out_map: float32 [2, 2, 32, 16, 32], P(None, None, 'tp'), may hold values from -2 to 2
- skip_weight: bfloat16 [2, 512], P(None, 'tp'), may hold values from -6 to 6
- gate_mix: bfloat16 [2, 32, 16, 16], P(None, 'tp'), may hold values from -1.5 to 1.5
- residual: bfloat16 [8192, 2048], P(('sp', 'tp')), may hold values from -6 to 6
- mixer_gain: float32 [1024], replicated, may hold values from 0.1 to 1.9
- out_proj: bfloat16 [1024, 2048], replicated, may hold values from -0.1875 to 0.1875
- ffn_gain: float32 [2048], replicated, may hold values from 0.1 to 1.9
- routes: int32 [8192, 2], P(('sp', 'tp')), may hold values from 0 to 127, all different within a row; in each aligned block of 64 rows (0 to 63, 64 to 127, ...) at most 2 rows name the same one
- route_weights: float32 [8192, 2], P(('sp', 'tp')), may hold values from 0.1 to 1
- gate_proj: bfloat16 [128, 2048, 1408], P(('sp', 'tp')), may hold values from -0.125 to 0.125
- up_proj: bfloat16 [128, 2048, 1408], P(('sp', 'tp')), may hold values from -0.125 to 0.125
- down_proj: bfloat16 [128, 1408, 2048], P(('sp', 'tp')), may hold values from -0.15625 to 0.15625
Outputs:
- layer_out: bfloat16 [8192, 2048], P(('sp', 'tp'))
The draws below stay inside these ranges and needn't reach their ends.
Inputs may be any that keep to these rules, and one draw needn't show every extreme that they name: `routes`: in each aligned block of 64 rows (the rows of one device), no expert is named by more than 2 entries, and the 2 experts of a row differ. `wide_poles`: along dimension 1, entry 0 (the real part) is negative and entry 1 (the imaginary part) is at least 0.1 in magnitude. `narrow_poles`: along dimension 1, entry 0 (the real part) is negative and entry 1 (the imaginary part) is at least 0.1 in magnitude. `step_sizes`: Positive.
All inputs are finite; a program needn't handle non-finite values.
Results may differ from the reference program's by a relative error of at most 0.014.
Values may be sent and summed in bfloat16 or wider, within the bound.
No kernel may reach another device: no remote copies, remote signals or barrier semaphores. Data moves between devices by JAX's collectives and lax.ppermute only.
A program may use at most 192 MiB of HBM per device.

```python
import math
import jax
import jax.numpy as jnp
import numpy as np
from jax import lax

D = 2048
GROUPS = 32
CHANNELS = 16
WIDE_STATE = 64
NARROW_STATE = 32
FE = 1408
TOP = 2
TOK_DEV = 128
TOKENS = 8192
ROWS = 64
SETW = 512
EXPERTS = 128
CAP = 2


def pick_slow(key):
    chance = 0.5
    return jax.random.bernoulli(jax.random.fold_in(key, 101), chance, (2, 2, GROUPS))


def make_poles(key, which, states):
    slow = pick_slow(key)[:, which]
    keys = jax.random.split(jax.random.fold_in(key, 11 + which), 4)
    slow_rate = jnp.exp(jax.random.uniform(keys[0], (2, GROUPS, states), jnp.float32, math.log(0.05), math.log(0.5))) / TOKENS
    fast_rate = jnp.exp(jax.random.uniform(keys[1], (2, GROUPS, states), jnp.float32, math.log(0.02), math.log(0.1)))
    decay_re = -jnp.where(slow[:, :, None], slow_rate, fast_rate)
    signs = jnp.where(jax.random.bernoulli(keys[3], 0.5, (2, GROUPS, states)), 1.0, -1.0)
    decay_im = jax.random.uniform(keys[2], (2, GROUPS, states), jnp.float32, 0.1, 3.14) * signs
    return jnp.stack([decay_re, decay_im], axis=1).astype(jnp.float32)


def draw_wide_poles(key, part):
    return make_poles(key, 0, WIDE_STATE)


def draw_narrow_poles(key, part):
    return make_poles(key, 1, NARROW_STATE)


def draw_step_sizes(key, part):
    slow = pick_slow(key)
    base = jnp.exp(jax.random.uniform(jax.random.fold_in(key, 21), (2, 2, GROUPS), jnp.float32, math.log(0.5), math.log(2.0)))
    return (base * jnp.where(slow, math.sqrt(0.4 / TOKENS), 0.3)).astype(jnp.float32)


def draw_forget(key, part):
    keys = jax.random.split(jax.random.fold_in(key, 31), 3)
    blocks = TOKENS // TOK_DEV
    factor = jnp.exp(jax.random.uniform(keys[0], (2, 2, GROUPS, blocks), jnp.float32, math.log(0.1), math.log(1.0)))
    decay_speed = jnp.repeat(factor, TOK_DEV, axis=3) / TOKENS
    spots = jax.random.randint(keys[1], (2, 2, GROUPS, 3), 0, TOKENS)
    total_quantity = jax.random.uniform(keys[2], (2, 2, GROUPS, 3), jnp.float32, 0.22, 0.69)
    slot_positions = jnp.arange(TOKENS)[None, None, None, None, :] == spots[:, :, :, :, None]
    signal_segments = jnp.sum(jnp.where(slot_positions, total_quantity[:, :, :, :, None], 0.0), axis=3)
    return (decay_speed + signal_segments).astype(jnp.float32)


def block_levels(stream_key, extent, cuts, least, top_value):
    factor_of = 1.0
    for position, parts in cuts:
        heights = jax.random.uniform(jax.random.fold_in(jax.random.fold_in(stream_key, 6), position), (parts,), jnp.float32, least / len(cuts), top_value / len(cuts))
        factor_of = factor_of * jnp.repeat(jnp.exp(heights), extent[position] // parts).reshape((-1,) + (1,) * (len(extent) - 1 - position))
    return factor_of


def assign_block(stream_key, own, number, rows, number_of, top, reach, skew):
    sequence = jax.random.permutation(stream_key, number_of)
    packed, common = shares(number_of, rows * top, reach, skew, True), shares(number_of, rows * top, reach, skew, False)
    places = jnp.arange(number_of)

    def named(tallies, rotation):
        used = int((tallies > 0).sum())
        fixed = max(1, used // 4)
        shifted = fixed + (places - fixed + rotation * (used - fixed)) % max(1, number_of - fixed)
        return jnp.zeros((number_of,), jnp.int32).at[sequence[jnp.where(places < fixed, places, shifted)]].set(jnp.asarray(tallies, jnp.int32))

    tallies = jnp.where(number % 4 == 0, named(packed, number // 4), named(common, number - number // 4 - 1))
    mixed = jax.random.permutation(jax.random.fold_in(own, 3), number_of)
    donor, sink = mixed[0:number_of // 2 * 2:2], mixed[1:number_of // 2 * 2:2]
    slack = jnp.minimum(tallies[donor] - 1, reach - tallies[sink]) // 2
    slack = jnp.where((donor == sequence[0]) | (sink == sequence[0]) | (tallies[sink] == 0), 0, jnp.maximum(slack, 0))
    shifted = jax.random.randint(jax.random.fold_in(own, 4), (number_of // 2,), 0, 1 << 20) % (slack + 1)
    tallies = tallies.at[donor].add(-shifted).at[sink].add(shifted)
    labels = jnp.searchsorted(jnp.cumsum(tallies), jnp.arange(rows * top), side="right").astype(jnp.int32)
    table = labels.reshape(top, rows).T
    table = table[jax.random.permutation(jax.random.fold_in(own, 1), rows)]
    rotation = jax.random.randint(jax.random.fold_in(own, 2), (rows, 1), 0, top)
    return jnp.take_along_axis(table, (jnp.arange(top)[None, :] + rotation) % top, axis=1)


def shares(count, total, bound, lean, full):
    weights = [(1 << 20) // math.isqrt(rank ** lean) + 1 for rank in range(1, count + 1)]
    largest = bound if full else min(bound, max(-(-total // count), total * weights[0] // sum(weights)))
    least = 1 if total - largest >= count - 1 else 0
    counts, spare = [largest] + [least] * (count - 1), total - largest - least * (count - 1)
    while spare > 0:
        candidates = [i for i in range(1, count) if counts[i] < largest] or [i for i in range(1, count) if counts[i] < bound]
        pool, left = sum([weights[i] for i in candidates]), spare
        for i in candidates:
            more = min(bound - counts[i], max(1, left * weights[i] // pool), spare)
            counts[i] = counts[i] + more
            spare = spare - more
    return np.array(counts)


def normal_values(key, shape, spread, reach, cuts=(), kind=jnp.bfloat16):
    values = spread * jax.random.normal(key, shape, jnp.float32)
    if cuts:
        values = values * block_levels(key, shape, cuts, -0.22, 0.18)
    return jnp.clip(values, -reach, reach).astype(kind)


def setup_inputs(seed: int = 0) -> dict:
    key_list = jax.random.split(jax.random.key(seed), 22)
    wide_inputs = normal_values(key_list[0], (TOKENS, SETW), 1.0, 6.0, ((0, 64), (1, 2)))
    narrow_inputs = normal_values(key_list[1], (TOKENS, SETW), 1.0, 6.0, ((0, 64), (1, 2)))
    wide_poles = draw_wide_poles(jax.random.fold_in(key_list[21], 71), 0)
    narrow_poles = draw_narrow_poles(jax.random.fold_in(key_list[21], 71), 0)
    step_sizes = draw_step_sizes(jax.random.fold_in(key_list[21], 71), 0)
    forget = draw_forget(jax.random.fold_in(key_list[21], 71), 0)
    wide_in_map = normal_values(key_list[6], (2, 2, GROUPS, CHANNELS, WIDE_STATE), ((2 * CHANNELS) ** -0.5), 2.5, ((2, 2),), jnp.float32)
    narrow_in_map = normal_values(key_list[7], (2, 2, GROUPS, CHANNELS, NARROW_STATE), ((2 * CHANNELS) ** -0.5), 2.5, ((2, 2),), jnp.float32)
    wide_out_map = normal_values(key_list[8], (2, 2, GROUPS, CHANNELS, WIDE_STATE), ((2 * WIDE_STATE) ** -0.5), 1.25, ((2, 2),), jnp.float32)
    narrow_out_map = normal_values(key_list[9], (2, 2, GROUPS, CHANNELS, NARROW_STATE), ((2 * NARROW_STATE) ** -0.5), 2.0, ((2, 2),), jnp.float32)
    skip_weight = normal_values(key_list[10], (2, SETW), 1.0, 6.0, ((1, 2),))
    gate_mix = normal_values(key_list[11], (2, GROUPS, CHANNELS, CHANNELS), CHANNELS ** -0.5, 1.5, ((1, 2),))
    residual = normal_values(key_list[12], (TOKENS, D), 1.0, 6.0, ((0, 128),))
    mixer_gain = jnp.clip(1.0 + 0.18 * jax.random.normal(key_list[13], (2 * SETW,), jnp.float32), 0.1, 1.9)
    out_proj = normal_values(key_list[14], (2 * SETW, D), (2 * SETW) ** -0.5, 0.1875)
    ffn_gain = jnp.clip(1.0 + 0.18 * jax.random.normal(key_list[15], (D,), jnp.float32), 0.1, 1.9)
    routes_keys = jax.random.split(jax.random.fold_in(key_list[16], 1), TOKENS // ROWS)
    routes_turns = jax.random.permutation(jax.random.fold_in(key_list[16], 3), TOKENS // ROWS)
    routes = jax.vmap(lambda own, number: assign_block(jax.random.fold_in(key_list[16], 2), own, number, ROWS, EXPERTS, TOP, CAP, 2))(routes_keys, routes_turns).reshape((TOKENS, TOP))
    route_weights = jnp.clip(jnp.exp(math.log(1.0) - 2.3025851 * jax.random.uniform(key_list[17], (TOKENS, TOP), jnp.float32) ** block_levels(key_list[17], (TOKENS, TOP), ((0, 128),), -0.2, 0.2)), 0.1, 1.0)
    gate_proj = normal_values(key_list[18], (EXPERTS, D, FE), D ** -0.5, 0.125, ((0, 128),))
    up_proj = normal_values(key_list[19], (EXPERTS, D, FE), D ** -0.5, 0.125, ((0, 128),))
    down_proj = normal_values(key_list[20], (EXPERTS, FE, D), FE ** -0.5, 0.15625, ((0, 128),))
    return dict(wide_inputs=wide_inputs, narrow_inputs=narrow_inputs, wide_poles=wide_poles, narrow_poles=narrow_poles, step_sizes=step_sizes, forget=forget, wide_in_map=wide_in_map, narrow_in_map=narrow_in_map, wide_out_map=wide_out_map, narrow_out_map=narrow_out_map, skip_weight=skip_weight, gate_mix=gate_mix, residual=residual, mixer_gain=mixer_gain, out_proj=out_proj, ffn_gain=ffn_gain, routes=routes, route_weights=route_weights, gate_proj=gate_proj, up_proj=up_proj, down_proj=down_proj)


maximum_value = lax.Precision.HIGHEST
epsilon = 1e-06

def pair_step(first, second):
    first_ar, first_ai, first_br, first_bi = first
    second_ar, second_ai, second_br, second_bi = second
    return (second_ar * first_ar - second_ai * first_ai, second_ar * first_ai + second_ai * first_ar, second_ar * first_br - second_ai * first_bi + second_br, second_ar * first_bi + second_ai * first_br + second_bi)

def block_diagonal_in(matrix):
    groups, channels, states = matrix.shape
    identity = jnp.eye(groups, dtype=jnp.float32)
    return jnp.einsum('gcs,gh->gchs', matrix, identity).reshape(groups * channels, groups * states)

def block_diagonal_out(matrix):
    groups, channels, states = matrix.shape
    identity = jnp.eye(groups, dtype=jnp.float32)
    return jnp.einsum('gcs,gh->gshc', matrix, identity).reshape(groups * states, groups * channels)

def local_states(input_sequence, poles, step, decay, in_map, backward):
    decay_re = poles[0]
    decay_im = poles[1]
    states = decay_re.shape[1]
    growth = jnp.exp(decay_re)
    numer_re = growth * jnp.cos(decay_im) - 1.0
    numer_im = growth * jnp.sin(decay_im)
    denom = decay_re * decay_re + decay_im * decay_im
    factor_re = (numer_re * decay_re + numer_im * decay_im) / denom * step[:, None]
    factor_im = (numer_im * decay_re - numer_re * decay_im) / denom * step[:, None]
    input_real = factor_re[:, None, :] * in_map[0] - factor_im[:, None, :] * in_map[1]
    input_imaginary = factor_re[:, None, :] * in_map[1] + factor_im[:, None, :] * in_map[0]
    driven_real = jnp.dot(input_sequence, block_diagonal_in(input_real), precision=maximum_value)
    driven_imaginary = jnp.dot(input_sequence, block_diagonal_in(input_imaginary), precision=maximum_value)
    flat_re = decay_re.reshape(-1)[None]
    flat_im = decay_im.reshape(-1)[None]
    magnitude = jnp.exp(flat_re - jnp.repeat(jnp.transpose(decay), states, axis=1))
    return lax.associative_scan(pair_step, (magnitude * jnp.cos(flat_im), magnitude * jnp.sin(flat_im), driven_real, driven_imaginary), reverse=backward, axis=0)

def read_out(hidden_state_real, hidden_state_imaginary, output_matrix):
    return jnp.dot(hidden_state_real, block_diagonal_out(output_matrix[0]), precision=maximum_value) - jnp.dot(hidden_state_imaginary, block_diagonal_out(output_matrix[1]), precision=maximum_value)

def finish_set(input_sequence, total, skip_row, gate_block):
    shaped = total + skip_row.astype(jnp.float32)[None] * input_sequence
    active = jax.nn.gelu(shaped, approximate=True)
    gate_full = block_diagonal_in(gate_block.astype(jnp.float32))
    opened = jax.nn.sigmoid(jnp.dot(active, gate_full, precision=maximum_value))
    return (active * opened).astype(jnp.bfloat16)

def run_set(inputs, poles, steps, decay, in_map, output_matrix, skip_row, gate_block):
    blocks = TOKENS // TOK_DEV
    groups = poles.shape[2]
    states = poles.shape[3]
    input_sequence = inputs.astype(jnp.float32)
    signal_blocks = input_sequence.reshape(blocks, TOK_DEV, groups * CHANNELS)
    total = jnp.zeros((TOKENS, groups * CHANNELS), jnp.float32)
    for direction in range(2):
        decay_blocks = jnp.transpose(decay[direction].reshape(groups, blocks, TOK_DEV), (1, 0, 2))
        backward = direction == 1
        edge = 0 if backward else -1

        def stepper(carry, pieces):
            piece, piece_decay = pieces
            prod_re, prod_im, hidden_state_real, hidden_state_imaginary = local_states(piece, poles[direction], steps[direction], piece_decay, in_map[direction], backward)
            full_re = hidden_state_real + prod_re * carry[0][None] - prod_im * carry[1][None]
            full_im = hidden_state_imaginary + prod_re * carry[1][None] + prod_im * carry[0][None]
            return ((full_re[edge], full_im[edge]), read_out(full_re, full_im, output_matrix[direction]))
        start = (jnp.zeros((groups * states,), jnp.float32), jnp.zeros((groups * states,), jnp.float32))
        _, outputs = lax.scan(stepper, start, (signal_blocks, decay_blocks), reverse=backward)
        total = total + outputs.reshape(TOKENS, groups * CHANNELS)
    return finish_set(input_sequence, total, skip_row, gate_block)

def reference(wide_inputs, narrow_inputs, wide_poles, narrow_poles, step_sizes, forget, wide_in_map, narrow_in_map, wide_out_map, narrow_out_map, skip_weight, gate_mix, residual, mixer_gain, out_proj, ffn_gain, routes, route_weights, gate_proj, up_proj, down_proj):
    wide_mix = run_set(wide_inputs, wide_poles, step_sizes[:, 0], forget[:, 0], wide_in_map, wide_out_map, skip_weight[0], gate_mix[0])
    narrow_mix = run_set(narrow_inputs, narrow_poles, step_sizes[:, 1], forget[:, 1], narrow_in_map, narrow_out_map, skip_weight[1], gate_mix[1])
    joined = jnp.concatenate([wide_mix, narrow_mix], axis=1).astype(jnp.float32)
    scale = lax.rsqrt(lax.optimization_barrier(jnp.mean(joined * joined, axis=1, keepdims=True)) + epsilon)
    mixed = (joined * scale * mixer_gain).astype(jnp.bfloat16)
    projected = jnp.dot(mixed, out_proj, preferred_element_type=jnp.float32)
    hidden1 = (residual.astype(jnp.float32) + projected).astype(jnp.bfloat16)
    hidden_wide = hidden1.astype(jnp.float32)
    normed = (hidden_wide * lax.rsqrt(lax.optimization_barrier(jnp.mean(hidden_wide * hidden_wide, axis=1, keepdims=True)) + epsilon) * ffn_gain).astype(jnp.bfloat16)
    share = route_weights / lax.optimization_barrier(jnp.sum(route_weights, axis=1, keepdims=True))
    blocks = TOKENS // ROWS
    picks = routes.reshape(blocks, ROWS * TOP)
    onehot = (picks[:, :, None] == jnp.arange(EXPERTS, dtype=jnp.int32)[None, None, :]).astype(jnp.int32)
    rank = lax.optimization_barrier(jnp.sum((jnp.cumsum(onehot, axis=1) - onehot) * onehot, axis=2))
    anchor = (jnp.arange(blocks, dtype=jnp.int32) * CAP)[:, None]
    place = (picks * (blocks * CAP) + anchor + rank).reshape(-1).astype(jnp.int32)
    sectioning = jnp.zeros((EXPERTS * blocks * CAP, D), jnp.bfloat16).at[place].set(jnp.repeat(normed, TOP, axis=0))

    def apply_expert(pieces):
        rows_in, gate_w, up_w, down_w = pieces
        gate_val = jnp.dot(rows_in, gate_w, preferred_element_type=jnp.float32)
        up_val = jnp.dot(rows_in, up_w, preferred_element_type=jnp.float32)
        expert_hidden = (jax.nn.silu(gate_val) * up_val).astype(jnp.bfloat16)
        return jnp.dot(expert_hidden, down_w, preferred_element_type=jnp.float32).astype(jnp.bfloat16)
    served = lax.map(apply_expert, (sectioning.reshape(EXPERTS, blocks * CAP, D), gate_proj, up_proj, down_proj))
    taken = jnp.take(served.reshape(-1, D), place, axis=0).reshape(TOKENS, TOP, D).astype(jnp.float32)
    result = hidden1.astype(jnp.float32) + lax.optimization_barrier(jnp.sum(share[:, :, None] * taken, axis=1))
    return result.astype(jnp.bfloat16)
```

```python
import functools

import jax
import jax.numpy as jnp
from jax import lax
from jax.experimental import pallas as pl
from jax.experimental.pallas import tpu as pltpu
from jax.sharding import Mesh
from jax.sharding import PartitionSpec as P

SP = ("sp_0", "sp_1", "sp_2")
SP_TP = ("sp_0", "sp_1", "sp_2", "tp")
EPS = 1e-06
F32 = jnp.float32
BF16 = jnp.bfloat16
T = 128
LANES = 128
NT = (((1,), (1,)), ((), ()))
WIDE = (8, 2, 64)
NARROW = (4, 4, 32)


def lane_ids(shape):
    return lax.broadcasted_iota(jnp.int32, shape, len(shape) - 1)


def in_rows(grouped, kind):
    rows, parts, _ = kind
    return jnp.concatenate([grouped[rows * h : rows * (h + 1)] for h in range(parts)], axis=1)


def side_by_side(pieces, row, kind):
    rows, parts, _ = kind
    return jnp.concatenate([pieces[row + rows * h] for h in range(parts)], axis=1)


def padded8(rows):
    if rows.shape[0] == 8:
        return rows
    return jnp.concatenate([rows, jnp.zeros((8 - rows.shape[0], LANES), F32)], axis=0)


def discretized(poles_ref, d):
    pr, pi = poles_ref[d, 0], poles_ref[d, 1]
    growth = jnp.exp(pr)
    cr, ci = growth * jnp.cos(pi), growth * jnp.sin(pi)
    nr = cr - 1.0
    denom = pr * pr + pi * pi
    fr = (nr * pr + ci * pi) / denom
    fi = (ci * pr - nr * pi) / denom
    return cr, ci, fr, fi


def group_block(row, r, kind):
    rows, parts, states = kind
    ids = (lane_ids(row.shape) % LANES) // states
    zeros = lambda n: [jnp.zeros((n, 2 * LANES), BF16)] if n else []
    row = row.astype(F32)
    out, at = [], 0
    for h in range(parts):
        start = 16 * (r + rows * h)
        out += zeros(start - at) + [jnp.where(ids == h, row, 0.0).astype(BF16)]
        at = start + 16
    return jnp.concatenate(out + zeros(16 * 16 - at), axis=0)


def spread(table, base, r, kind):
    rows, parts, states = kind
    n = table.shape[0]
    lanes = lane_ids((n, LANES)) // states
    out = jnp.broadcast_to(table[:, base + r : base + r + 1], (n, LANES))
    for h in range(1, parts):
        k = base + r + rows * h
        out = jnp.where(lanes == h, jnp.broadcast_to(table[:, k : k + 1], (n, LANES)), out)
    return out


def push_into(steps_ref, which, d, u, poles_ref, in_ref, kind, re_ref, im_ref):
    rows, parts, _ = kind
    cr, ci, fr, fi = discretized(poles_ref, d)
    for r in range(rows):
        re, im = [], []
        for h in range(parts):
            g = r + rows * h
            step = steps_ref[(d * 2 + which) * 16 + g]
            gr, gi = fr[g : g + 1] * step, fi[g : g + 1] * step
            br, bi = in_ref[d, 0, g], in_ref[d, 1, g]
            re.append(gr * br - gi * bi)
            im.append(gr * bi + gi * br)
        row = jnp.concatenate([jnp.concatenate(re, axis=1), jnp.concatenate(im, axis=1)], axis=1)
        driven = jnp.dot(u, group_block(row, r, kind), preferred_element_type=F32)
        re_ref[pl.ds(r, T, stride=8), :] = driven[:, :LANES]
        im_ref[pl.ds(r, T, stride=8), :] = driven[:, LANES:]
    return padded8(in_rows(cr, kind)), padded8(in_rows(ci, kind))


def forget_columns(forget_ref):
    both = forget_ref[...]
    return jnp.transpose(jnp.concatenate([both, both], axis=0))


def load_pushes(steps_ref, u_refs, pole_refs, in_refs, forget_t, scr):
    kept = jnp.exp(-forget_t)
    turns = []
    for d in range(2):
        for which, kind in ((0, WIDE), (1, NARROW)):
            re_ref, im_ref, e_ref = scr[(d * 2 + which) * 3 : (d * 2 + which) * 3 + 3]
            if kind is NARROW:
                for ref in (re_ref, im_ref, e_ref):
                    ref[...] = jnp.zeros((8 * T, LANES), F32)
            for r in range(kind[0]):
                e_ref[pl.ds(r, T, stride=8), :] = spread(kept, (d * 2 + which) * 16, r, kind)
            turns.append(
                push_into(
                    steps_ref, which, d, u_refs[which][...], pole_refs[which], in_refs[which],
                    kind, re_ref, im_ref,
                )
            )
    return turns


def three_terms(x):
    hi = x.astype(BF16).astype(F32)
    mid = (x - hi).astype(BF16).astype(F32)
    return hi, mid, x - hi - mid


def ends_kernel(
    me_ref, steps_ref, wu_ref, nu_ref, wp_ref, np_ref, wi_ref, ni_ref, forget_ref, send_ref, *scr
):
    forget_t = forget_columns(forget_ref)
    turns = load_pushes(
        steps_ref, (wu_ref, nu_ref), (wp_ref, np_ref), (wi_ref, ni_ref), forget_t, scr
    )

    def step(t, state):
        new = []
        for k in range(4):
            re_ref, im_ref, e_ref = scr[3 * k : 3 * k + 3]
            at = pl.multiple_of((t if k < 2 else T - 1 - t) * 8, 8)
            (cr, ci), (sr, si) = turns[k], state[k]
            e = e_ref[pl.ds(at, 8), :]
            new.append(
                (
                    e * (cr * sr - ci * si) + re_ref[pl.ds(at, 8), :],
                    e * (cr * si + ci * sr) + im_ref[pl.ds(at, 8), :],
                )
            )
        return tuple(new)

    zero = jnp.zeros((8, LANES), F32)
    state = lax.fori_loop(0, T, step, ((zero, zero),) * 4, unroll=8)
    kept = jnp.exp(-jnp.sum(forget_t, axis=0, keepdims=True))
    hi, mid, lo = three_terms(kept)
    first = lane_ids((1, LANES)) < 64
    terms = jnp.where(first, hi, mid)
    rest = jnp.where(first, lo, 0.0)
    row = lax.broadcasted_iota(jnp.int32, (8, LANES), 0)
    blocks = []
    for d in range(2):
        (wr, wi), (nr, ni) = state[2 * d], state[2 * d + 1]
        nr = jnp.where(row < 4, nr, jnp.where(row == 4, terms, jnp.where(row == 5, rest, 0.0)))
        blocks.append(jnp.concatenate([wr, wi, nr, jnp.where(row < 4, ni, 0.0)], axis=0))
    me = me_ref[0]

    def put(j, _):
        at = pl.multiple_of(j * 32, 32)
        send_ref[pl.ds(at, 32), :] = jnp.where(j > me, blocks[0], blocks[1]).astype(BF16)
        return 0

    lax.fori_loop(0, send_ref.shape[0] // 32, put, 0)


def read_blocks(out_ref, d, r, kind):
    return side_by_side(out_ref[d, 0], r, kind), side_by_side(out_ref[d, 1], r, kind)


def local_kernel(
    steps_ref, wu_ref, nu_ref, wp_ref, np_ref, wi_ref, ni_ref, forget_ref, wo_ref, no_ref, after_ref,
    y_ref, decay_ref, *scr
):
    del after_ref
    turns = load_pushes(
        steps_ref, (wu_ref, nu_ref), (wp_ref, np_ref), (wi_ref, ni_ref),
        forget_columns(forget_ref), scr,
    )
    prods = scr[12:]

    def step(t, state):
        new = []
        for k in range(4):
            re_ref, im_ref, e_ref = scr[3 * k : 3 * k + 3]
            at = pl.ds(pl.multiple_of((t if k < 2 else T - 1 - t) * 8, 8), 8)
            (cr, ci), (sr, si, pr, pi) = turns[k], state[k]
            e = e_ref[at, :]
            got = (
                e * (cr * sr - ci * si) + re_ref[at, :],
                e * (cr * si + ci * sr) + im_ref[at, :],
                e * (cr * pr - ci * pi),
                e * (cr * pi + ci * pr),
            )
            re_ref[at, :], im_ref[at, :] = got[0], got[1]
            prods[2 * k][at, :], prods[2 * k + 1][at, :] = got[2], got[3]
            new.append(got)
        return tuple(new)

    zero = jnp.zeros((8, LANES), F32)
    lax.fori_loop(0, T, step, ((zero, zero, zero + 1.0, zero),) * 4, unroll=4)
    for which, (kind, out_ref) in enumerate(((WIDE, wo_ref), (NARROW, no_ref))):
        total = jnp.zeros((T, 2 * LANES), F32)
        for d in range(2):
            k = d * 2 + which
            for r in range(kind[0]):
                at = pl.ds(r, T, stride=8)
                o_re, o_im = read_blocks(out_ref, d, r, kind)
                weights = group_block(jnp.concatenate([o_re, -o_im], axis=1), r, kind)
                hidden = jnp.concatenate([scr[3 * k][at, :], scr[3 * k + 1][at, :]], axis=1)
                total += lax.dot_general(
                    hidden.astype(BF16), weights, NT, preferred_element_type=F32
                )
                decay = jnp.concatenate([prods[2 * k][at, :], prods[2 * k + 1][at, :]], axis=1)
                first = ((d * 12) + which * 8 + r) * 2 * LANES
                decay_ref[:, first : first + 2 * LANES] = decay.astype(BF16)
        y_ref[:, which * 2 * LANES : (which + 1) * 2 * LANES] = total


def carry_kernel(
    me_ref, got_ref, wu_ref, nu_ref, wp_ref, np_ref, wo_ref, no_ref, y_ref, decay_ref, skip_ref,
    gate_ref, out_ref, flat, *kept
):
    me = me_ref[0]
    blocks = got_ref.shape[0] // 32
    flat[...] = got_ref[...].astype(F32)
    first = flat[pl.ds(20, blocks, stride=32), :]
    table = first + pltpu.roll(first, 64, 1) + flat[pl.ds(21, blocks, stride=32), :]
    turns = []
    for d in range(2):
        for which, (kind, poles_ref) in enumerate(((WIDE, wp_ref), (NARROW, np_ref))):
            k = d * 2 + which
            if kind is NARROW:
                kept[k][...] = jnp.zeros((8 * blocks, LANES), F32)
            for r in range(kind[0]):
                kept[k][pl.ds(r, blocks, stride=8), :] = spread(table, k * 16, r, kind)
            pr, pi = poles_ref[d, 0], poles_ref[d, 1]
            growth = jnp.exp(pr)
            cr, ci = growth * jnp.cos(pi), growth * jnp.sin(pi)
            for _ in range(7):
                cr, ci = cr * cr - ci * ci, 2.0 * cr * ci
            turns.append((padded8(in_rows(cr, kind)), padded8(in_rows(ci, kind))))

    def step(i, state):
        new = []
        for k in range(4):
            j = i if k < 2 else blocks - 1 - i
            used = (j < me) if k < 2 else (j > me)
            base = pl.multiple_of(j * 32, 32)
            re_at, im_at = (0, 8) if k % 2 == 0 else (16, 24)
            (cr, ci), (sr, si) = turns[k], state[k]
            e = kept[k][pl.ds(pl.multiple_of(j * 8, 8), 8), :]
            re = e * (cr * sr - ci * si) + flat[pl.ds(base + re_at, 8), :]
            im = e * (cr * si + ci * sr) + flat[pl.ds(base + im_at, 8), :]
            new.append((jnp.where(used, re, sr), jnp.where(used, im, si)))
        return tuple(new)

    zero = jnp.zeros((8, LANES), F32)
    state = lax.fori_loop(0, blocks, step, ((zero, zero),) * 4, unroll=4)
    for which, (kind, u_ref, o_ref) in enumerate(((WIDE, wu_ref, wo_ref), (NARROW, nu_ref, no_ref))):
        span = slice(which * 2 * LANES, (which + 1) * 2 * LANES)
        total = y_ref[:, span]
        for d in range(2):
            sr, si = state[d * 2 + which]
            for r in range(kind[0]):
                o_re, o_im = read_blocks(o_ref, d, r, kind)
                cr, ci = sr[r : r + 1], si[r : r + 1]
                row = jnp.concatenate([o_re * cr - o_im * ci, -(o_re * ci + o_im * cr)], axis=1)
                at = ((d * 12) + which * 8 + r) * 2 * LANES
                total += lax.dot_general(
                    decay_ref[:, at : at + 2 * LANES], group_block(row, r, kind), NT,
                    preferred_element_type=F32,
                )
        shaped = total + skip_ref[which : which + 1].astype(F32) * u_ref[...].astype(F32)
        inner = 0.7978845608028654 * (shaped + 0.044715 * (shaped * shaped * shaped))
        active = 0.5 * shaped * (1.0 + jnp.tanh(inner))
        hi = active.astype(BF16)
        lo = (active - hi.astype(F32)).astype(BF16)
        line = gate_ref[which].astype(F32)
        ids = lane_ids(line.shape) // 16
        gate = jnp.concatenate(
            [jnp.where(ids == g, line, 0.0).astype(BF16) for g in range(16)], axis=0
        )
        mixed = jnp.dot(hi, gate, preferred_element_type=F32) + jnp.dot(
            lo, gate, preferred_element_type=F32
        )
        out_ref[:, span] = (active * jax.nn.sigmoid(mixed)).astype(BF16)


SMEM = pl.BlockSpec(memory_space=pltpu.SMEM)
VMEM = pl.BlockSpec(memory_space=pltpu.VMEM)


def column(n):
    return pltpu.VMEM((8 * n, LANES), F32)


def mixer(me, wide_u, narrow_u, wide_p, narrow_p, steps, forget, wide_in, narrow_in, wide_out,
          narrow_out, skip, gate):
    blocks = lax.axis_size(SP)
    steps = steps.reshape(-1)
    forget = forget.reshape(-1, T)
    params = pltpu.CompilerParams(vmem_limit_bytes=32 * 2**20)
    shared = (wide_u, narrow_u, wide_p, narrow_p, wide_in, narrow_in, forget)
    send = pl.pallas_call(
        ends_kernel,
        out_shape=jax.ShapeDtypeStruct((blocks * 32, LANES), BF16),
        in_specs=[SMEM, SMEM] + [VMEM] * 7,
        out_specs=VMEM,
        scratch_shapes=[column(T)] * 12,
        compiler_params=params,
        name="ends",
    )(me, steps, *shared)
    got = lax.all_to_all(
        send.reshape(blocks, 32, LANES), SP, split_axis=0, concat_axis=0, tiled=True
    )
    y, decay = pl.pallas_call(
        local_kernel,
        out_shape=(
            jax.ShapeDtypeStruct((T, 4 * LANES), F32),
            jax.ShapeDtypeStruct((T, 24 * 2 * LANES), BF16),
        ),
        in_specs=[SMEM] + [VMEM] * 9 + [pl.BlockSpec(memory_space=pl.ANY)],
        out_specs=(VMEM, VMEM),
        scratch_shapes=[column(T)] * 20,
        compiler_params=params,
        name="local",
    )(steps, *shared, wide_out, narrow_out, send)
    return pl.pallas_call(
        carry_kernel,
        out_shape=jax.ShapeDtypeStruct((T, 4 * LANES), BF16),
        in_specs=[SMEM] + [VMEM] * 11,
        out_specs=VMEM,
        scratch_shapes=[pltpu.VMEM((blocks * 32, LANES), F32)] + [column(blocks)] * 4,
        compiler_params=params,
        name="carry",
    )(me, got.reshape(-1, LANES), wide_u, narrow_u, wide_p, narrow_p, wide_out, narrow_out, y,
      decay, skip, gate)


def ranks(routes):
    rows = routes.shape[0]
    earlier = jnp.arange(rows)[None, :] < jnp.arange(rows)[:, None]
    out = []
    for k in range(2):
        same = sum(
            (routes[:, k][:, None] == routes[:, o][None, :]).astype(jnp.int32) for o in range(2)
        )
        out.append(jnp.sum(jnp.where(earlier, same, 0), axis=1))
    return out


def local(
    wide_inputs, narrow_inputs, wide_poles, narrow_poles, step_sizes, forget, wide_in_map,
    narrow_in_map, wide_out_map, narrow_out_map, skip_weight, gate_mix, residual, mixer_gain,
    out_proj, ffn_gain, routes, route_weights, gate_proj, up_proj, down_proj,
):
    me = lax.axis_index(SP).astype(jnp.int32).reshape(1)
    gate_rows = jnp.transpose(gate_mix, (0, 2, 1, 3)).reshape(2, 16, 256)
    set_out = mixer(
        me, wide_inputs, narrow_inputs, wide_poles, narrow_poles, step_sizes, forget, wide_in_map,
        narrow_in_map, wide_out_map, narrow_out_map, skip_weight, gate_rows,
    )
    rows = residual.shape[0]
    width = residual.shape[1]
    both = lax.all_to_all(
        set_out.reshape(2, rows, 512), "tp", split_axis=0, concat_axis=0, tiled=True
    )
    joined = jnp.concatenate(
        [both[0, :, :256], both[1, :, :256], both[0, :, 256:], both[1, :, 256:]], axis=1
    ).astype(F32)
    scale = lax.rsqrt(jnp.mean(joined * joined, axis=1, keepdims=True) + EPS)
    mixed = (joined * scale * mixer_gain).astype(BF16)
    projected = jnp.dot(mixed, out_proj, preferred_element_type=F32)
    hidden1 = (residual.astype(F32) + projected).astype(BF16)
    hidden_wide = hidden1.astype(F32)
    normed = (
        hidden_wide
        * lax.rsqrt(jnp.mean(hidden_wide * hidden_wide, axis=1, keepdims=True) + EPS)
        * ffn_gain
    ).astype(BF16)
    experts = lax.axis_size(SP) * lax.axis_size("tp")
    place = [routes[:, k] * 2 + rank for k, rank in enumerate(ranks(routes))]
    slots = jnp.arange(2 * experts, dtype=jnp.int32)
    picks = [(slots[None, :] == at[:, None]).astype(BF16) for at in place]
    sections = lax.dot_general(
        picks[0] + picks[1], normed, (((0,), (0,)), ((), ())), preferred_element_type=F32
    ).astype(BF16)
    arrived = lax.all_to_all(
        sections.reshape(experts, 2, width), SP_TP, split_axis=0, concat_axis=0, tiled=True
    ).reshape(-1, width)
    gate_val = jnp.dot(arrived, gate_proj[0], preferred_element_type=F32)
    up_val = jnp.dot(arrived, up_proj[0], preferred_element_type=F32)
    expert_hidden = (jax.nn.silu(gate_val) * up_val).astype(BF16)
    done = jnp.dot(expert_hidden, down_proj[0], preferred_element_type=F32).astype(BF16)
    returned = lax.all_to_all(
        done.reshape(experts, 2, width), SP_TP, split_axis=0, concat_axis=0, tiled=True
    ).reshape(-1, width)
    share = route_weights / jnp.sum(route_weights, axis=1, keepdims=True)
    result = hidden_wide
    for k in range(2):
        taken = jnp.dot(picks[k], returned, preferred_element_type=F32)
        result = result + share[:, k : k + 1] * taken
    return result.astype(BF16)


def solution(mesh):
    finer = Mesh(mesh.devices.reshape(4, 4, 4, mesh.shape["tp"]), SP_TP)
    return jax.shard_map(
        local,
        mesh=finer,
        in_specs=(
            P(SP, "tp"),
            P(SP, "tp"),
            P(None, None, "tp", None),
            P(None, None, "tp", None),
            P(None, None, "tp"),
            P(None, None, "tp", SP),
            P(None, None, "tp", None, None),
            P(None, None, "tp", None, None),
            P(None, None, "tp", None, None),
            P(None, None, "tp", None, None),
            P(None, "tp"),
            P(None, "tp", None, None),
            P(SP_TP, None),
            P(),
            P(),
            P(),
            P(SP_TP, None),
            P(SP_TP, None),
            P(SP_TP, None, None),
            P(SP_TP, None, None),
            P(SP_TP, None, None),
        ),
        out_specs=P(SP_TP, None),
        check_vma=False,
    )
```

```python
import functools

import jax
import jax.numpy as jnp
from jax import lax
from jax.experimental import pallas as pl
from jax.experimental.pallas import tpu as pltpu
from jax.sharding import Mesh
from jax.sharding import PartitionSpec as P

SP = ("sp_0", "sp_1", "sp_2")
SP_TP = ("sp_0", "sp_1", "sp_2", "tp")
EPS = 1e-06
F32 = jnp.float32
BF16 = jnp.bfloat16
T = 128
LANES = 128
NT = (((1,), (1,)), ((), ()))
WIDE = (8, 2, 64)
NARROW = (4, 4, 32)


def started(sources, buffers, sems):
    copies = [
        pltpu.make_async_copy(source, buffer, sems.at[k])
        for k, (source, buffer) in enumerate(zip(sources, buffers))
    ]
    for copy in copies:
        copy.start()
    return copies


def fetch(sources, buffers, sems):
    for copy in started(sources, buffers, sems):
        copy.wait()


def lane_ids(shape):
    return lax.broadcasted_iota(jnp.int32, shape, len(shape) - 1)


def in_rows(grouped, kind):
    rows, parts, _ = kind
    return jnp.concatenate([grouped[rows * h : rows * (h + 1)] for h in range(parts)], axis=1)


def side_by_side(pieces, row, kind):
    rows, parts, _ = kind
    return jnp.concatenate([pieces[row + rows * h] for h in range(parts)], axis=1)


def padded8(rows):
    if rows.shape[0] == 8:
        return rows
    return jnp.concatenate([rows, jnp.zeros((8 - rows.shape[0], LANES), F32)], axis=0)


def discretized(poles_ref, d):
    pr, pi = poles_ref[d, 0], poles_ref[d, 1]
    growth = jnp.exp(pr)
    cr, ci = growth * jnp.cos(pi), growth * jnp.sin(pi)
    nr = cr - 1.0
    denom = pr * pr + pi * pi
    fr = (nr * pr + ci * pi) / denom
    fi = (ci * pr - nr * pi) / denom
    return cr, ci, fr, fi


def group_block(row, r, kind):
    rows, parts, states = kind
    ids = (lane_ids(row.shape) % LANES) // states
    zeros = lambda n: [jnp.zeros((n, 2 * LANES), BF16)] if n else []
    row = row.astype(F32)
    out, at = [], 0
    for h in range(parts):
        start = 16 * (r + rows * h)
        out += zeros(start - at) + [jnp.where(ids == h, row, 0.0).astype(BF16)]
        at = start + 16
    return jnp.concatenate(out + zeros(16 * 16 - at), axis=0)


def spread(table, base, r, kind):
    rows, parts, states = kind
    n = table.shape[0]
    lanes = lane_ids((n, LANES)) // states
    out = jnp.broadcast_to(table[:, base + r : base + r + 1], (n, LANES))
    for h in range(1, parts):
        k = base + r + rows * h
        out = jnp.where(lanes == h, jnp.broadcast_to(table[:, k : k + 1], (n, LANES)), out)
    return out


def push_into(steps_ref, which, d, u, poles_ref, in_ref, kind, re_ref, im_ref):
    rows, parts, _ = kind
    cr, ci, fr, fi = discretized(poles_ref, d)
    for r in range(rows):
        re, im = [], []
        for h in range(parts):
            g = r + rows * h
            step = steps_ref[(d * 2 + which) * 16 + g]
            gr, gi = fr[g : g + 1] * step, fi[g : g + 1] * step
            br, bi = in_ref[d, 0, g], in_ref[d, 1, g]
            re.append(gr * br - gi * bi)
            im.append(gr * bi + gi * br)
        row = jnp.concatenate([jnp.concatenate(re, axis=1), jnp.concatenate(im, axis=1)], axis=1)
        driven = jnp.dot(u, group_block(row, r, kind), preferred_element_type=F32)
        re_ref[pl.ds(r, T, stride=8), :] = driven[:, :LANES]
        im_ref[pl.ds(r, T, stride=8), :] = driven[:, LANES:]
    return padded8(in_rows(cr, kind)), padded8(in_rows(ci, kind))


def forget_columns(forget_ref):
    both = forget_ref[...]
    return jnp.transpose(jnp.concatenate([both, both], axis=0))


def load_pushes(steps_ref, u_refs, pole_refs, in_refs, forget_t, scr):
    kept = jnp.exp(-forget_t)
    turns = []
    for d in range(2):
        for which, kind in ((0, WIDE), (1, NARROW)):
            re_ref, im_ref, e_ref = scr[(d * 2 + which) * 3 : (d * 2 + which) * 3 + 3]
            if kind is NARROW:
                for ref in (re_ref, im_ref, e_ref):
                    ref[...] = jnp.zeros((8 * T, LANES), F32)
            for r in range(kind[0]):
                e_ref[pl.ds(r, T, stride=8), :] = spread(kept, (d * 2 + which) * 16, r, kind)
            turns.append(
                push_into(
                    steps_ref, which, d, u_refs[which][...], pole_refs[which], in_refs[which],
                    kind, re_ref, im_ref,
                )
            )
    return turns


def three_terms(x):
    hi = x.astype(BF16).astype(F32)
    mid = (x - hi).astype(BF16).astype(F32)
    return hi, mid, x - hi - mid


def ends_kernel(me_ref, steps_ref, *refs):
    sources, send_ref, buffers, sems, scr = refs[:7], refs[7], refs[8:15], refs[15], refs[16:]
    fetch(sources, buffers, sems)
    wu_ref, nu_ref, wp_ref, np_ref, wi_ref, ni_ref, forget_ref = buffers
    forget_t = forget_columns(forget_ref)
    turns = load_pushes(
        steps_ref, (wu_ref, nu_ref), (wp_ref, np_ref), (wi_ref, ni_ref), forget_t, scr
    )

    def step(t, state):
        new = []
        for k in range(4):
            re_ref, im_ref, e_ref = scr[3 * k : 3 * k + 3]
            at = pl.multiple_of((t if k < 2 else T - 1 - t) * 8, 8)
            (cr, ci), (sr, si) = turns[k], state[k]
            e = e_ref[pl.ds(at, 8), :]
            new.append(
                (
                    e * (cr * sr - ci * si) + re_ref[pl.ds(at, 8), :],
                    e * (cr * si + ci * sr) + im_ref[pl.ds(at, 8), :],
                )
            )
        return tuple(new)

    zero = jnp.zeros((8, LANES), F32)
    state = lax.fori_loop(0, T, step, ((zero, zero),) * 4, unroll=8)
    kept = jnp.exp(-jnp.sum(forget_t, axis=0, keepdims=True))
    hi, mid, lo = three_terms(kept)
    first = lane_ids((1, LANES)) < 64
    terms = jnp.where(first, hi, mid)
    rest = jnp.where(first, lo, 0.0)
    row = lax.broadcasted_iota(jnp.int32, (8, LANES), 0)
    blocks = []
    for d in range(2):
        (wr, wi), (nr, ni) = state[2 * d], state[2 * d + 1]
        nr = jnp.where(row < 4, nr, jnp.where(row == 4, terms, jnp.where(row == 5, rest, 0.0)))
        blocks.append(jnp.concatenate([wr, wi, nr, jnp.where(row < 4, ni, 0.0)], axis=0))
    me = me_ref[0]

    def put(j, _):
        at = pl.multiple_of(j * 32, 32)
        send_ref[pl.ds(at, 32), :] = jnp.where(j > me, blocks[0], blocks[1]).astype(BF16)
        return 0

    lax.fori_loop(0, send_ref.shape[0] // 32, put, 0)


def read_blocks(out_ref, d, r, kind):
    return side_by_side(out_ref[d, 0], r, kind), side_by_side(out_ref[d, 1], r, kind)


def local_kernel(steps_ref, *refs):
    sources, results, buffers = refs[:9], refs[10:12], refs[12:21]
    sems, y_ref, decay_ref, out_sems, scr = refs[21], refs[22], refs[23], refs[24], refs[25:]
    fetch(sources, buffers, sems)
    wu_ref, nu_ref, wp_ref, np_ref, wi_ref, ni_ref, forget_ref, wo_ref, no_ref = buffers
    turns = load_pushes(
        steps_ref, (wu_ref, nu_ref), (wp_ref, np_ref), (wi_ref, ni_ref),
        forget_columns(forget_ref), scr,
    )
    prods = scr[12:]

    def step(t, state):
        new = []
        for k in range(4):
            re_ref, im_ref, e_ref = scr[3 * k : 3 * k + 3]
            at = pl.ds(pl.multiple_of((t if k < 2 else T - 1 - t) * 8, 8), 8)
            (cr, ci), (sr, si, pr, pi) = turns[k], state[k]
            e = e_ref[at, :]
            got = (
                e * (cr * sr - ci * si) + re_ref[at, :],
                e * (cr * si + ci * sr) + im_ref[at, :],
                e * (cr * pr - ci * pi),
                e * (cr * pi + ci * pr),
            )
            re_ref[at, :], im_ref[at, :] = got[0], got[1]
            prods[2 * k][at, :], prods[2 * k + 1][at, :] = got[2], got[3]
            new.append(got)
        return tuple(new)

    zero = jnp.zeros((8, LANES), F32)
    lax.fori_loop(0, T, step, ((zero, zero, zero + 1.0, zero),) * 4, unroll=4)
    for which, (kind, out_ref) in enumerate(((WIDE, wo_ref), (NARROW, no_ref))):
        total = jnp.zeros((T, 2 * LANES), F32)
        for d in range(2):
            k = d * 2 + which
            for r in range(kind[0]):
                at = pl.ds(r, T, stride=8)
                o_re, o_im = read_blocks(out_ref, d, r, kind)
                weights = group_block(jnp.concatenate([o_re, -o_im], axis=1), r, kind)
                hidden = jnp.concatenate([scr[3 * k][at, :], scr[3 * k + 1][at, :]], axis=1)
                total += lax.dot_general(
                    hidden.astype(BF16), weights, NT, preferred_element_type=F32
                )
                decay = jnp.concatenate([prods[2 * k][at, :], prods[2 * k + 1][at, :]], axis=1)
                first = ((d * 12) + which * 8 + r) * 2 * LANES
                decay_ref[:, first : first + 2 * LANES] = decay.astype(BF16)
        y_ref[:, which * 2 * LANES : (which + 1) * 2 * LANES] = total
    fetch((y_ref, decay_ref), results, out_sems)


def carry_kernel(me_ref, got_ref, *refs):
    sources, out_ref, weights_ref, buffers = refs[:11], refs[11], refs[12], refs[13:23]
    sems, flat, kept = refs[23], refs[24], refs[25:]
    copies = started(sources, buffers + (weights_ref,), sems)
    wp_ref, np_ref, wu_ref, nu_ref, wo_ref, no_ref, skip_ref, gate_ref, y_ref, decay_ref = buffers
    for copy in copies[:2]:
        copy.wait()
    me = me_ref[0]
    blocks = got_ref.shape[0] // 32
    flat[...] = got_ref[...].astype(F32)
    first = flat[pl.ds(20, blocks, stride=32), :]
    table = first + pltpu.roll(first, 64, 1) + flat[pl.ds(21, blocks, stride=32), :]
    turns = []
    for d in range(2):
        for which, (kind, poles_ref) in enumerate(((WIDE, wp_ref), (NARROW, np_ref))):
            k = d * 2 + which
            if kind is NARROW:
                kept[k][...] = jnp.zeros((8 * blocks, LANES), F32)
            for r in range(kind[0]):
                kept[k][pl.ds(r, blocks, stride=8), :] = spread(table, k * 16, r, kind)
            pr, pi = poles_ref[d, 0], poles_ref[d, 1]
            growth = jnp.exp(pr)
            cr, ci = growth * jnp.cos(pi), growth * jnp.sin(pi)
            for _ in range(7):
                cr, ci = cr * cr - ci * ci, 2.0 * cr * ci
            turns.append((padded8(in_rows(cr, kind)), padded8(in_rows(ci, kind))))

    def step(i, state):
        new = []
        for k in range(4):
            j = i if k < 2 else blocks - 1 - i
            used = (j < me) if k < 2 else (j > me)
            base = pl.multiple_of(j * 32, 32)
            re_at, im_at = (0, 8) if k % 2 == 0 else (16, 24)
            (cr, ci), (sr, si) = turns[k], state[k]
            e = kept[k][pl.ds(pl.multiple_of(j * 8, 8), 8), :]
            re = e * (cr * sr - ci * si) + flat[pl.ds(base + re_at, 8), :]
            im = e * (cr * si + ci * sr) + flat[pl.ds(base + im_at, 8), :]
            new.append((jnp.where(used, re, sr), jnp.where(used, im, si)))
        return tuple(new)

    zero = jnp.zeros((8, LANES), F32)
    state = lax.fori_loop(0, blocks, step, ((zero, zero),) * 4, unroll=4)
    for copy in copies[2:10]:
        copy.wait()
    for which, (kind, u_ref, o_ref) in enumerate(((WIDE, wu_ref, wo_ref), (NARROW, nu_ref, no_ref))):
        span = slice(which * 2 * LANES, (which + 1) * 2 * LANES)
        total = y_ref[:, span]
        for d in range(2):
            sr, si = state[d * 2 + which]
            for r in range(kind[0]):
                o_re, o_im = read_blocks(o_ref, d, r, kind)
                cr, ci = sr[r : r + 1], si[r : r + 1]
                row = jnp.concatenate([o_re * cr - o_im * ci, -(o_re * ci + o_im * cr)], axis=1)
                at = ((d * 12) + which * 8 + r) * 2 * LANES
                total += lax.dot_general(
                    decay_ref[:, at : at + 2 * LANES], group_block(row, r, kind), NT,
                    preferred_element_type=F32,
                )
        shaped = total + skip_ref[which : which + 1].astype(F32) * u_ref[...].astype(F32)
        inner = 0.7978845608028654 * (shaped + 0.044715 * (shaped * shaped * shaped))
        active = 0.5 * shaped * (1.0 + jnp.tanh(inner))
        hi = active.astype(BF16)
        lo = (active - hi.astype(F32)).astype(BF16)
        line = gate_ref[which].astype(F32)
        ids = lane_ids(line.shape) // 16
        gate = jnp.concatenate(
            [jnp.where(ids == g, line, 0.0).astype(BF16) for g in range(16)], axis=0
        )
        mixed = jnp.dot(hi, gate, preferred_element_type=F32) + jnp.dot(
            lo, gate, preferred_element_type=F32
        )
        out_ref[:, span] = (active * jax.nn.sigmoid(mixed)).astype(BF16)
    copies[10].wait()


SMEM = pl.BlockSpec(memory_space=pltpu.SMEM)
VMEM = pl.BlockSpec(memory_space=pltpu.VMEM)
HBM = pl.BlockSpec(memory_space=pltpu.HBM)
MIB = 2**20


def column(n):
    return pltpu.VMEM((8 * n, LANES), F32)


def fetched(arrays):
    return [pltpu.VMEM(a.shape, a.dtype) for a in arrays] + [
        pltpu.SemaphoreType.DMA((len(arrays),))
    ]


def far(arrays):
    return tuple(pltpu.with_memory_space_constraint(a, pltpu.HBM) for a in arrays)


def grant(mib):
    return pltpu.CompilerParams(vmem_limit_bytes=mib * MIB)


def mixer(me, wide_u, narrow_u, wide_p, narrow_p, steps, forget, wide_in, narrow_in, wide_out,
          narrow_out, skip, gate, out_proj):
    blocks = lax.axis_size(SP)
    steps = steps.reshape(-1)
    forget = forget.reshape(-1, T)
    shared = far((wide_u, narrow_u, wide_p, narrow_p, wide_in, narrow_in, forget))
    send = pl.pallas_call(
        ends_kernel,
        out_shape=jax.ShapeDtypeStruct((blocks * 32, LANES), BF16),
        in_specs=[SMEM, SMEM] + [HBM] * 7,
        out_specs=VMEM,
        scratch_shapes=fetched(shared) + [column(T)] * 12,
        compiler_params=grant(20),
        name="ends",
    )(me, steps, *shared)
    got = lax.all_to_all(
        send.reshape(blocks, 32, LANES), SP, split_axis=0, concat_axis=0, tiled=True
    )
    sources = shared + far((wide_out, narrow_out))
    y, decay = pl.pallas_call(
        local_kernel,
        out_shape=(
            pltpu.HBM((T, 4 * LANES), F32),
            pltpu.HBM((T, 24 * 2 * LANES), BF16),
        ),
        in_specs=[SMEM] + [HBM] * 10,
        out_specs=(HBM, HBM),
        scratch_shapes=fetched(sources)
        + [pltpu.VMEM((T, 4 * LANES), F32), pltpu.VMEM((T, 24 * 2 * LANES), BF16)]
        + [pltpu.SemaphoreType.DMA((2,))] + [column(T)] * 20,
        compiler_params=grant(24),
        name="local",
    )(steps, *sources, send)
    sources = far(
        (wide_p, narrow_p, wide_u, narrow_u, wide_out, narrow_out, skip, gate, y, decay, out_proj)
    )
    return pl.pallas_call(
        carry_kernel,
        out_shape=(
            jax.ShapeDtypeStruct((T, 4 * LANES), BF16),
            jax.ShapeDtypeStruct(out_proj.shape, BF16),
        ),
        in_specs=[SMEM, VMEM] + [HBM] * 11,
        out_specs=(VMEM, VMEM),
        scratch_shapes=[pltpu.VMEM(a.shape, a.dtype) for a in sources[:10]]
        + [pltpu.SemaphoreType.DMA((11,))]
        + [pltpu.VMEM((blocks * 32, LANES), F32)] + [column(blocks)] * 4,
        compiler_params=grant(20),
        name="carry",
    )(me, got.reshape(-1, LANES), *sources)


def project_kernel(
    core_ref, mine_ref, other_ref, rows_ref, gain_ref, ffn_ref, residual_ref, proj_ref, hidden_ref,
    send_ref,
):
    swap = core_ref[0] == 1
    mine, other = mine_ref[...].astype(F32), other_ref[...].astype(F32)
    first, second = jnp.where(swap, other, mine), jnp.where(swap, mine, other)
    half = first.shape[1] // 2
    joined = jnp.concatenate(
        [first[:, :half], second[:, :half], first[:, half:], second[:, half:]], axis=1
    )
    scale = lax.rsqrt(jnp.mean(joined * joined, axis=1, keepdims=True) + EPS)
    mixed = (joined * scale * gain_ref[...]).astype(BF16)
    projected = jnp.dot(mixed, proj_ref[...], preferred_element_type=F32)
    hidden1 = (residual_ref[...].astype(F32) + projected).astype(BF16)
    hidden_ref[...] = hidden1
    wide = hidden1.astype(F32)
    scale = lax.rsqrt(jnp.mean(wide * wide, axis=1, keepdims=True) + EPS)
    normed = (wide * scale * ffn_ref[...]).astype(BF16)
    quarter = normed.shape[1] // 4
    stacked = jnp.concatenate([normed[:, q * quarter : (q + 1) * quarter] for q in range(4)], axis=0)
    size = stacked.shape[0]
    for b in range(send_ref.shape[0] // size):
        ids = lax.broadcasted_iota(jnp.int32, (size, size), 0) + b * size
        hit = (ids == rows_ref[0:1, :]) | (ids == rows_ref[1:2, :])
        pick = jnp.where(hit, 1.0, 0.0).astype(BF16)
        send_ref[b * size : (b + 1) * size, :] = jnp.dot(
            pick, stacked, preferred_element_type=F32
        ).astype(BF16)


def turned(back):
    out = lax.broadcasted_iota(jnp.int32, (256, 256), 0)
    src = lax.broadcasted_iota(jnp.int32, (256, 256), 1)
    if back:
        out, src = src, out
    wanted = ((out % 64) // 2) * 8 + (out // 64) * 2 + out % 2
    return jnp.where(src == wanted, 1.0, 0.0).astype(BF16)


def experts_kernel(
    in_ref, gate_ref, up_ref, far_ref, out_ref, x_ref, h_ref, down_ref, sem
):
    copy = pltpu.make_async_copy(far_ref, down_ref, sem)
    copy.start()
    quarter = in_ref.shape[1]
    turn = turned(False)
    for b in range(4):
        got = jnp.dot(
            turn, in_ref[b * 256 : (b + 1) * 256, :], preferred_element_type=F32
        ).astype(BF16)
        for q in range(4):
            x_ref[b * 64 : (b + 1) * 64, q * quarter : (q + 1) * quarter] = got[
                q * 64 : (q + 1) * 64
            ]
    x = x_ref[...]
    gate = jnp.dot(x, gate_ref[...], preferred_element_type=F32)
    up = jnp.dot(x, up_ref[...], preferred_element_type=F32)
    h_ref[...] = (gate * jax.nn.sigmoid(gate) * up).astype(BF16)
    copy.wait()
    done = jnp.dot(h_ref[...], down_ref[...], preferred_element_type=F32).astype(BF16)
    back = turned(True)
    for b in range(4):
        stacked = jnp.concatenate(
            [
                done[b * 64 : (b + 1) * 64, q * quarter : (q + 1) * quarter] for q in range(4)
            ],
            axis=0,
        )
        out_ref[b * 256 : (b + 1) * 256, :] = jnp.dot(
            back, stacked, preferred_element_type=F32
        ).astype(BF16)


def combine_kernel(got_ref, cols_ref, weights_ref, hidden_ref, out_ref):
    w = weights_ref[...]
    total = w[:, 0:1] + w[:, 1:2]
    rows = hidden_ref.shape[0]
    quarter = got_ref.shape[1]
    size = got_ref.shape[0]
    got = got_ref[...]
    result = hidden_ref[...].astype(F32)
    ids = lax.broadcasted_iota(jnp.int32, (4 * rows, size), 1)
    for k in range(2):
        pick = jnp.where(ids == cols_ref[:, k : k + 1], 1.0, 0.0).astype(BF16)
        taken = jnp.dot(pick, got, preferred_element_type=F32)
        taken = jnp.concatenate([taken[q * rows : (q + 1) * rows] for q in range(4)], axis=1)
        result = result + (w[:, k : k + 1] / total) * taken
    out_ref[...] = result.astype(BF16)


def ranks(routes):
    rows = routes.shape[0]
    earlier = jnp.arange(rows)[None, :] < jnp.arange(rows)[:, None]
    out = []
    for k in range(2):
        same = sum(
            (routes[:, k][:, None] == routes[:, o][None, :]).astype(jnp.int32) for o in range(2)
        )
        out.append(jnp.sum(jnp.where(earlier, same, 0), axis=1))
    return out


def local(
    wide_inputs, narrow_inputs, wide_poles, narrow_poles, step_sizes, forget, wide_in_map,
    narrow_in_map, wide_out_map, narrow_out_map, skip_weight, gate_mix, residual, mixer_gain,
    out_proj, ffn_gain, routes, route_weights, gate_proj, up_proj, down_proj,
):
    me = lax.axis_index(SP).astype(jnp.int32).reshape(1)
    gate_rows = jnp.transpose(gate_mix, (0, 2, 1, 3)).reshape(2, 16, 256)
    set_out, near_proj = mixer(
        me, wide_inputs, narrow_inputs, wide_poles, narrow_poles, step_sizes, forget, wide_in_map,
        narrow_in_map, wide_out_map, narrow_out_map, skip_weight, gate_rows, out_proj,
    )
    rows = residual.shape[0]
    width = residual.shape[1]
    core = lax.axis_index("tp").astype(jnp.int32)
    halves = set_out.reshape(2, rows, 512)
    mine = lax.dynamic_index_in_dim(halves, core, 0, keepdims=False)
    other = lax.dynamic_index_in_dim(halves, 1 - core, 0, keepdims=False)
    other = lax.ppermute(other, "tp", [(0, 1), (1, 0)])
    experts = lax.axis_size(SP) * lax.axis_size("tp")
    quarters = jnp.repeat(jnp.arange(4, dtype=jnp.int32) * 2, rows)
    places = jnp.stack(
        [jnp.tile(routes[:, k] * 8 + rank, 4) + quarters for k, rank in enumerate(ranks(routes))]
    )
    hidden1, send = pl.pallas_call(
        project_kernel,
        out_shape=(
            jax.ShapeDtypeStruct((rows, width), BF16),
            jax.ShapeDtypeStruct((experts * 8, width // 4), BF16),
        ),
        in_specs=[SMEM] + [VMEM] * 7,
        out_specs=(VMEM, VMEM),
        compiler_params=grant(12),
        name="project",
    )(
        core.reshape(1), mine, other, places, mixer_gain.reshape(1, -1), ffn_gain.reshape(1, -1),
        residual, near_proj,
    )
    exchange = lambda x: lax.all_to_all(
        x.reshape(experts, 8, width // 4), SP_TP, split_axis=0, concat_axis=0, tiled=True
    ).reshape(-1, width // 4)
    done = pl.pallas_call(
        experts_kernel,
        out_shape=jax.ShapeDtypeStruct((experts * 8, width // 4), BF16),
        in_specs=[VMEM] * 3 + [HBM],
        out_specs=VMEM,
        scratch_shapes=[
            pltpu.VMEM((2 * experts, width), BF16),
            pltpu.VMEM((2 * experts, gate_proj.shape[2]), BF16),
            pltpu.VMEM(down_proj.shape[1:], BF16),
            pltpu.SemaphoreType.DMA,
        ],
        compiler_params=grant(20),
        name="experts",
    )(exchange(send), gate_proj[0], up_proj[0], *far((down_proj[0],)))
    return pl.pallas_call(
        combine_kernel,
        out_shape=jax.ShapeDtypeStruct((rows, width), BF16),
        in_specs=[VMEM] * 4,
        out_specs=VMEM,
        compiler_params=grant(12),
        name="combine",
    )(exchange(done), places.T, route_weights, hidden1)


def solution(mesh):
    finer = Mesh(mesh.devices.reshape(4, 4, 4, mesh.shape["tp"]), SP_TP)
    return jax.shard_map(
        local,
        mesh=finer,
        in_specs=(
            P(SP, "tp"),
            P(SP, "tp"),
            P(None, None, "tp", None),
            P(None, None, "tp", None),
            P(None, None, "tp"),
            P(None, None, "tp", SP),
            P(None, None, "tp", None, None),
            P(None, None, "tp", None, None),
            P(None, None, "tp", None, None),
            P(None, None, "tp", None, None),
            P(None, "tp"),
            P(None, "tp", None, None),
            P(SP_TP, None),
            P(),
            P(),
            P(),
            P(SP_TP, None),
            P(SP_TP, None),
            P(SP_TP, None, None),
            P(SP_TP, None, None),
            P(SP_TP, None, None),
        ),
        out_specs=P(SP_TP, None),
        check_vma=False,
    )
```

```python
import functools

import jax
import jax.numpy as jnp
from jax import lax
from jax.experimental import pallas as pl
from jax.experimental.pallas import tpu as pltpu
from jax.sharding import Mesh
from jax.sharding import PartitionSpec as P

SP = ("sp_0", "sp_1", "sp_2")
SP_TP = ("sp_0", "sp_1", "sp_2", "tp")
EPS = 1e-06
F32 = jnp.float32
BF16 = jnp.bfloat16
T = 128
LANES = 128
NT = (((1,), (1,)), ((), ()))
WIDE = (8, 2, 64)
NARROW = (4, 4, 32)


def started(sources, buffers, sems):
    copies = [
        pltpu.make_async_copy(source, buffer, sems.at[k])
        for k, (source, buffer) in enumerate(zip(sources, buffers))
    ]
    for copy in copies:
        copy.start()
    return copies


def lane_ids(shape):
    return lax.broadcasted_iota(jnp.int32, shape, len(shape) - 1)


def in_rows(grouped, kind):
    rows, parts, _ = kind
    return jnp.concatenate([grouped[rows * h : rows * (h + 1)] for h in range(parts)], axis=1)


def side_by_side(pieces, row, kind):
    rows, parts, _ = kind
    return jnp.concatenate([pieces[row + rows * h] for h in range(parts)], axis=1)


def padded8(rows):
    if rows.shape[0] == 8:
        return rows
    return jnp.concatenate([rows, jnp.zeros((8 - rows.shape[0], LANES), F32)], axis=0)


def discretized(poles_ref, d):
    pr, pi = poles_ref[d, 0], poles_ref[d, 1]
    growth = jnp.exp(pr)
    cr, ci = growth * jnp.cos(pi), growth * jnp.sin(pi)
    nr = cr - 1.0
    denom = pr * pr + pi * pi
    fr = (nr * pr + ci * pi) / denom
    fi = (ci * pr - nr * pi) / denom
    return cr, ci, fr, fi


def group_block(row, r, kind):
    rows, parts, states = kind
    ids = (lane_ids(row.shape) % LANES) // states
    zeros = lambda n: [jnp.zeros((n, 2 * LANES), BF16)] if n else []
    row = row.astype(F32)
    out, at = [], 0
    for h in range(parts):
        start = 16 * (r + rows * h)
        out += zeros(start - at) + [jnp.where(ids == h, row, 0.0).astype(BF16)]
        at = start + 16
    return jnp.concatenate(out + zeros(16 * 16 - at), axis=0)


def spread(table, base, r, kind):
    rows, parts, states = kind
    n = table.shape[0]
    lanes = lane_ids((n, LANES)) // states
    out = jnp.broadcast_to(table[:, base + r : base + r + 1], (n, LANES))
    for h in range(1, parts):
        k = base + r + rows * h
        out = jnp.where(lanes == h, jnp.broadcast_to(table[:, k : k + 1], (n, LANES)), out)
    return out


def push_into(steps_ref, which, d, u, poles_ref, in_ref, kind, re_ref, im_ref):
    rows, parts, _ = kind
    cr, ci, fr, fi = discretized(poles_ref, d)
    for r in range(rows):
        re, im = [], []
        for h in range(parts):
            g = r + rows * h
            step = steps_ref[d, which, g]
            gr, gi = fr[g : g + 1] * step, fi[g : g + 1] * step
            br, bi = in_ref[d, 0, g], in_ref[d, 1, g]
            re.append(gr * br - gi * bi)
            im.append(gr * bi + gi * br)
        row = jnp.concatenate([jnp.concatenate(re, axis=1), jnp.concatenate(im, axis=1)], axis=1)
        driven = jnp.dot(u, group_block(row, r, kind), preferred_element_type=F32)
        re_ref[pl.ds(r, T, stride=8), :] = driven[:, :LANES]
        im_ref[pl.ds(r, T, stride=8), :] = driven[:, LANES:]
    return padded8(in_rows(cr, kind)), padded8(in_rows(ci, kind))


def forget_columns(forget_ref):
    both = forget_ref[...]
    return jnp.transpose(jnp.concatenate([both, both], axis=0))


def load_pushes(copies, buffers, scr):
    wu_ref, nu_ref, wp_ref, np_ref, wi_ref, ni_ref, forget_ref, steps_ref = buffers
    copies[6].wait()
    forget_t = forget_columns(forget_ref)
    kept = jnp.exp(-forget_t)
    sets = ((WIDE, wu_ref, wp_ref, wi_ref), (NARROW, nu_ref, np_ref, ni_ref))
    for d in range(2):
        for which in range(2):
            k = d * 2 + which
            kind = sets[which][0]
            re_ref, im_ref, e_ref = scr[3 * k : 3 * k + 3]
            if kind is NARROW:
                for ref in (re_ref, im_ref, e_ref):
                    ref[...] = jnp.zeros((8 * T, LANES), F32)
            for r in range(kind[0]):
                e_ref[pl.ds(r, T, stride=8), :] = spread(kept, k * 16, r, kind)
    for k in (0, 1, 2, 3, 4, 5, 7):
        copies[k].wait()
    turns = []
    for d in range(2):
        for which, (kind, u_ref, poles_ref, in_ref) in enumerate(sets):
            k = d * 2 + which
            re_ref, im_ref, _ = scr[3 * k : 3 * k + 3]
            turns.append(
                push_into(steps_ref, which, d, u_ref[...], poles_ref, in_ref, kind, re_ref, im_ref)
            )
    return turns, forget_t


def three_terms(x):
    hi = x.astype(BF16).astype(F32)
    mid = (x - hi).astype(BF16).astype(F32)
    return hi, mid, x - hi - mid


def ends_kernel(me_ref, *refs):
    sources, send_ref, buffers, sems, scr = refs[:8], refs[8], refs[9:17], refs[17], refs[18:]
    turns, forget_t = load_pushes(started(sources, buffers, sems), buffers, scr)

    def step(t, state):
        new = []
        for k in range(4):
            re_ref, im_ref, e_ref = scr[3 * k : 3 * k + 3]
            at = pl.multiple_of((t if k < 2 else T - 1 - t) * 8, 8)
            (cr, ci), (sr, si) = turns[k], state[k]
            e = e_ref[pl.ds(at, 8), :]
            new.append(
                (
                    e * (cr * sr - ci * si) + re_ref[pl.ds(at, 8), :],
                    e * (cr * si + ci * sr) + im_ref[pl.ds(at, 8), :],
                )
            )
        return tuple(new)

    zero = jnp.zeros((8, LANES), F32)
    state = lax.fori_loop(0, T, step, ((zero, zero),) * 4, unroll=8)
    kept = jnp.exp(-jnp.sum(forget_t, axis=0, keepdims=True))
    hi, mid, lo = three_terms(kept)
    first = lane_ids((1, LANES)) < 64
    terms = jnp.where(first, hi, mid)
    rest = jnp.where(first, lo, 0.0)
    row = lax.broadcasted_iota(jnp.int32, (8, LANES), 0)
    blocks = []
    for d in range(2):
        (wr, wi), (nr, ni) = state[2 * d], state[2 * d + 1]
        nr = jnp.where(row < 4, nr, jnp.where(row == 4, terms, jnp.where(row == 5, rest, 0.0)))
        blocks.append(jnp.concatenate([wr, wi, nr, jnp.where(row < 4, ni, 0.0)], axis=0))
    me = me_ref[0]

    def put(j, _):
        at = pl.multiple_of(j * 32, 32)
        send_ref[pl.ds(at, 32), :] = jnp.where(j > me, blocks[0], blocks[1]).astype(BF16)
        return 0

    lax.fori_loop(0, send_ref.shape[0] // 32, put, 0)


def read_blocks(out_ref, d, r, kind):
    return side_by_side(out_ref[d, 0], r, kind), side_by_side(out_ref[d, 1], r, kind)


def local_kernel(*refs):
    sources, results, buffers, sems = refs[:10], refs[11:13], refs[13:23], refs[23]
    y_ref, decay_ref, out_sems, scr = refs[24], refs[25], refs[26], refs[27:]
    copies = started(sources, buffers, sems)
    turns, _ = load_pushes(copies, buffers[:8], scr)
    wo_ref, no_ref = buffers[8:]
    prods = scr[12:]

    def step(t, state):
        new = []
        for k in range(4):
            re_ref, im_ref, e_ref = scr[3 * k : 3 * k + 3]
            at = pl.ds(pl.multiple_of((t if k < 2 else T - 1 - t) * 8, 8), 8)
            (cr, ci), (sr, si, pr, pi) = turns[k], state[k]
            e = e_ref[at, :]
            got = (
                e * (cr * sr - ci * si) + re_ref[at, :],
                e * (cr * si + ci * sr) + im_ref[at, :],
                e * (cr * pr - ci * pi),
                e * (cr * pi + ci * pr),
            )
            re_ref[at, :], im_ref[at, :] = got[0], got[1]
            prods[2 * k][at, :], prods[2 * k + 1][at, :] = got[2], got[3]
            new.append(got)
        return tuple(new)

    zero = jnp.zeros((8, LANES), F32)
    lax.fori_loop(0, T, step, ((zero, zero, zero + 1.0, zero),) * 4, unroll=4)
    copies[8].wait()
    copies[9].wait()
    for which, (kind, out_ref) in enumerate(((WIDE, wo_ref), (NARROW, no_ref))):
        total = jnp.zeros((T, 2 * LANES), F32)
        for d in range(2):
            k = d * 2 + which
            for r in range(kind[0]):
                at = pl.ds(r, T, stride=8)
                o_re, o_im = read_blocks(out_ref, d, r, kind)
                weights = group_block(jnp.concatenate([o_re, -o_im], axis=1), r, kind)
                hidden = jnp.concatenate([scr[3 * k][at, :], scr[3 * k + 1][at, :]], axis=1)
                total += lax.dot_general(
                    hidden.astype(BF16), weights, NT, preferred_element_type=F32
                )
                decay = jnp.concatenate([prods[2 * k][at, :], prods[2 * k + 1][at, :]], axis=1)
                first = ((d * 12) + which * 8 + r) * 2 * LANES
                decay_ref[:, first : first + 2 * LANES] = decay.astype(BF16)
        y_ref[:, which * 2 * LANES : (which + 1) * 2 * LANES] = total
    for copy in started((y_ref, decay_ref), results, out_sems):
        copy.wait()


def carry_kernel(me_ref, got_ref, *refs):
    sources, out_ref, weights_ref, buffers = refs[:11], refs[11], refs[12], refs[13:23]
    sems, flat, kept = refs[23], refs[24], refs[25:]
    copies = started(sources, buffers + (weights_ref,), sems)
    wp_ref, np_ref, wu_ref, nu_ref, wo_ref, no_ref, skip_ref, gate_ref, y_ref, decay_ref = buffers
    for copy in copies[:2]:
        copy.wait()
    me = me_ref[0]
    blocks = got_ref.shape[0] // 32
    flat[...] = got_ref[...].astype(F32)
    first = flat[pl.ds(20, blocks, stride=32), :]
    table = first + pltpu.roll(first, 64, 1) + flat[pl.ds(21, blocks, stride=32), :]
    turns = []
    for d in range(2):
        for which, (kind, poles_ref) in enumerate(((WIDE, wp_ref), (NARROW, np_ref))):
            k = d * 2 + which
            if kind is NARROW:
                kept[k][...] = jnp.zeros((8 * blocks, LANES), F32)
            for r in range(kind[0]):
                kept[k][pl.ds(r, blocks, stride=8), :] = spread(table, k * 16, r, kind)
            pr, pi = poles_ref[d, 0], poles_ref[d, 1]
            growth = jnp.exp(pr)
            cr, ci = growth * jnp.cos(pi), growth * jnp.sin(pi)
            for _ in range(7):
                cr, ci = cr * cr - ci * ci, 2.0 * cr * ci
            turns.append((padded8(in_rows(cr, kind)), padded8(in_rows(ci, kind))))

    def step(i, state):
        new = []
        for k in range(4):
            j = i if k < 2 else blocks - 1 - i
            used = (j < me) if k < 2 else (j > me)
            base = pl.multiple_of(j * 32, 32)
            re_at, im_at = (0, 8) if k % 2 == 0 else (16, 24)
            (cr, ci), (sr, si) = turns[k], state[k]
            e = kept[k][pl.ds(pl.multiple_of(j * 8, 8), 8), :]
            re = e * (cr * sr - ci * si) + flat[pl.ds(base + re_at, 8), :]
            im = e * (cr * si + ci * sr) + flat[pl.ds(base + im_at, 8), :]
            new.append((jnp.where(used, re, sr), jnp.where(used, im, si)))
        return tuple(new)

    zero = jnp.zeros((8, LANES), F32)
    state = lax.fori_loop(0, blocks, step, ((zero, zero),) * 4, unroll=4)
    for copy in copies[2:10]:
        copy.wait()
    for which, (kind, u_ref, o_ref) in enumerate(((WIDE, wu_ref, wo_ref), (NARROW, nu_ref, no_ref))):
        span = slice(which * 2 * LANES, (which + 1) * 2 * LANES)
        total = y_ref[:, span]
        for d in range(2):
            sr, si = state[d * 2 + which]
            for r in range(kind[0]):
                o_re, o_im = read_blocks(o_ref, d, r, kind)
                cr, ci = sr[r : r + 1], si[r : r + 1]
                row = jnp.concatenate([o_re * cr - o_im * ci, -(o_re * ci + o_im * cr)], axis=1)
                at = ((d * 12) + which * 8 + r) * 2 * LANES
                total += lax.dot_general(
                    decay_ref[:, at : at + 2 * LANES], group_block(row, r, kind), NT,
                    preferred_element_type=F32,
                )
        shaped = total + skip_ref[which : which + 1].astype(F32) * u_ref[...].astype(F32)
        inner = 0.7978845608028654 * (shaped + 0.044715 * (shaped * shaped * shaped))
        active = 0.5 * shaped * (1.0 + jnp.tanh(inner))
        hi = active.astype(BF16)
        lo = (active - hi.astype(F32)).astype(BF16)
        spread_out = jnp.where(
            lane_ids((16, 256)) % 16 == lax.broadcasted_iota(jnp.int32, (16, 256), 0), 1.0, 0.0
        ).astype(BF16)
        gate = jnp.dot(gate_ref[which], spread_out, preferred_element_type=F32)
        own = lax.broadcasted_iota(jnp.int32, (256, 256), 0) // 16 == lane_ids((256, 256)) // 16
        gate = jnp.where(own, gate, 0.0).astype(BF16)
        mixed = jnp.dot(hi, gate, preferred_element_type=F32) + jnp.dot(
            lo, gate, preferred_element_type=F32
        )
        out_ref[:, span] = (active * jax.nn.sigmoid(mixed)).astype(BF16)
    copies[10].wait()


SMEM = pl.BlockSpec(memory_space=pltpu.SMEM)
VMEM = pl.BlockSpec(memory_space=pltpu.VMEM)
HBM = pl.BlockSpec(memory_space=pltpu.HBM)
MIB = 2**20


def column(n):
    return pltpu.VMEM((8 * n, LANES), F32)


def fetched(arrays):
    return [
        (pltpu.SMEM if a.shape == (2, 2, 16) else pltpu.VMEM)(a.shape, a.dtype) for a in arrays
    ] + [pltpu.SemaphoreType.DMA((len(arrays),))]


def far(arrays):
    return tuple(pltpu.with_memory_space_constraint(a, pltpu.HBM) for a in arrays)


def cost(us):
    return pl.CostEstimate(flops=int(us * 1e9), bytes_accessed=int(us * 1e6), transcendentals=0)


def grant(mib):
    return pltpu.CompilerParams(vmem_limit_bytes=mib * MIB)


def mixer(me, wide_u, narrow_u, wide_p, narrow_p, steps, forget, wide_in, narrow_in, wide_out,
          narrow_out, skip, gate, out_proj):
    blocks = lax.axis_size(SP)
    forget = forget.reshape(-1, T)
    shared = far((wide_u, narrow_u, wide_p, narrow_p, wide_in, narrow_in, forget, steps))
    send = pl.pallas_call(
        ends_kernel,
        out_shape=jax.ShapeDtypeStruct((blocks * 32, LANES), BF16),
        in_specs=[SMEM] + [HBM] * 8,
        out_specs=VMEM,
        scratch_shapes=fetched(shared) + [column(T)] * 12,
        compiler_params=grant(20),
        cost_estimate=cost(6),
        name="ends",
    )(me, *shared)
    got = lax.all_to_all(
        send.reshape(blocks, 32, LANES), SP, split_axis=0, concat_axis=0, tiled=True
    )
    sources = shared + far((wide_out, narrow_out))
    y, decay = pl.pallas_call(
        local_kernel,
        out_shape=(
            pltpu.HBM((T, 4 * LANES), F32),
            pltpu.HBM((T, 24 * 2 * LANES), BF16),
        ),
        in_specs=[HBM] * 11,
        out_specs=(HBM, HBM),
        scratch_shapes=fetched(sources)
        + [pltpu.VMEM((T, 4 * LANES), F32), pltpu.VMEM((T, 24 * 2 * LANES), BF16)]
        + [pltpu.SemaphoreType.DMA((2,))] + [column(T)] * 20,
        compiler_params=grant(24),
        cost_estimate=cost(8),
        name="local",
    )(*sources, *far((send,)))
    sources = far(
        (wide_p, narrow_p, wide_u, narrow_u, wide_out, narrow_out, skip, gate, y, decay, out_proj)
    )
    return pl.pallas_call(
        carry_kernel,
        out_shape=(
            jax.ShapeDtypeStruct((T, 4 * LANES), BF16),
            jax.ShapeDtypeStruct(out_proj.shape, BF16),
        ),
        in_specs=[SMEM, VMEM] + [HBM] * 11,
        out_specs=(VMEM, VMEM),
        scratch_shapes=[pltpu.VMEM(a.shape, a.dtype) for a in sources[:10]]
        + [pltpu.SemaphoreType.DMA((11,))]
        + [pltpu.VMEM((blocks * 32, LANES), F32)] + [column(blocks)] * 4,
        compiler_params=grant(16),
        cost_estimate=cost(5),
        name="carry",
    )(me, got.reshape(-1, LANES), *sources)


def places(routes):
    n = routes.shape[1]
    flat = jnp.concatenate([routes, routes], axis=1).astype(F32)
    line = [flat[k : k + 1] for k in range(2)]
    first = lax.broadcasted_iota(jnp.int32, (2 * n, 2 * n), 0) == 0
    table = jnp.transpose(jnp.where(first, line[0], line[1]))
    lanes, rows = lane_ids((n, 2 * n)), lax.broadcasted_iota(jnp.int32, (n, 2 * n), 0)
    wide = [jnp.broadcast_to(table[:n, k : k + 1], (n, 2 * n)) for k in range(2)]
    across, down = [], []
    for k in range(2):
        over, under = 0.0, 0.0
        for o in range(2):
            over += jnp.where((rows < lanes % n) & (wide[o] == line[k]), 1.0, 0.0)
            under += jnp.where((lanes < rows) & (wide[k] == line[o]), 1.0, 0.0)
        at = line[k] * 8.0 + jnp.sum(over, axis=0, keepdims=True) + 2.0 * (lanes[:1] // n)
        across.append(jnp.concatenate([at, at + 4.0], axis=1).astype(jnp.int32))
        at = table[:n, k : k + 1] * 8.0 + jnp.sum(under, axis=1, keepdims=True)
        down.append(jnp.concatenate([at + 2.0 * q for q in range(4)], axis=0).astype(jnp.int32))
    return across, down


def project_kernel(
    core_ref, mine_ref, other_ref, routes_ref, gain_ref, ffn_ref, residual_ref, proj_ref,
    hidden_ref, send_ref, cols_ref,
):
    across, down = places(routes_ref[...])
    shape = cols_ref.shape
    cols_ref[...] = jnp.where(
        lane_ids(shape) == 0, jnp.broadcast_to(down[0], shape), jnp.broadcast_to(down[1], shape)
    )
    swap = core_ref[0] == 1
    mine, other = mine_ref[...].astype(F32), other_ref[...].astype(F32)
    first, second = jnp.where(swap, other, mine), jnp.where(swap, mine, other)
    half = first.shape[1] // 2
    joined = jnp.concatenate(
        [first[:, :half], second[:, :half], first[:, half:], second[:, half:]], axis=1
    )
    scale = lax.rsqrt(jnp.mean(joined * joined, axis=1, keepdims=True) + EPS)
    mixed = (joined * scale * gain_ref[...]).astype(BF16)
    projected = jnp.dot(mixed, proj_ref[...], preferred_element_type=F32)
    hidden1 = (residual_ref[...].astype(F32) + projected).astype(BF16)
    hidden_ref[...] = hidden1
    wide = hidden1.astype(F32)
    scale = lax.rsqrt(jnp.mean(wide * wide, axis=1, keepdims=True) + EPS)
    normed = (wide * scale * ffn_ref[...]).astype(BF16)
    quarter = normed.shape[1] // 4
    stacked = jnp.concatenate([normed[:, q * quarter : (q + 1) * quarter] for q in range(4)], axis=0)
    size = stacked.shape[0]
    for b in range(send_ref.shape[0] // size):
        ids = lax.broadcasted_iota(jnp.int32, (size, size), 0) + b * size
        hit = (ids == across[0]) | (ids == across[1])
        pick = jnp.where(hit, 1.0, 0.0).astype(BF16)
        send_ref[b * size : (b + 1) * size, :] = jnp.dot(
            pick, stacked, preferred_element_type=F32
        ).astype(BF16)


def turned(back):
    out = lax.broadcasted_iota(jnp.int32, (256, 256), 0)
    src = lax.broadcasted_iota(jnp.int32, (256, 256), 1)
    if back:
        out, src = src, out
    wanted = ((out % 64) // 2) * 8 + (out // 64) * 2 + out % 2
    return jnp.where(src == wanted, 1.0, 0.0).astype(BF16)


def experts_kernel(
    in_ref, gate_ref, up_ref, far_ref, out_ref, x_ref, h_ref, down_ref, sem
):
    copy = pltpu.make_async_copy(far_ref, down_ref, sem)
    copy.start()
    quarter = in_ref.shape[1]
    turn = turned(False)
    for b in range(4):
        got = jnp.dot(
            turn, in_ref[b * 256 : (b + 1) * 256, :], preferred_element_type=F32
        ).astype(BF16)
        for q in range(4):
            x_ref[b * 64 : (b + 1) * 64, q * quarter : (q + 1) * quarter] = got[
                q * 64 : (q + 1) * 64
            ]
    x = x_ref[...]
    gate = jnp.dot(x, gate_ref[...], preferred_element_type=F32)
    up = jnp.dot(x, up_ref[...], preferred_element_type=F32)
    h_ref[...] = (gate * jax.nn.sigmoid(gate) * up).astype(BF16)
    copy.wait()
    done = jnp.dot(h_ref[...], down_ref[...], preferred_element_type=F32).astype(BF16)
    back = turned(True)
    for b in range(4):
        stacked = jnp.concatenate(
            [
                done[b * 64 : (b + 1) * 64, q * quarter : (q + 1) * quarter] for q in range(4)
            ],
            axis=0,
        )
        out_ref[b * 256 : (b + 1) * 256, :] = jnp.dot(
            back, stacked, preferred_element_type=F32
        ).astype(BF16)


def combine_kernel(got_ref, cols_ref, weights_ref, hidden_ref, out_ref):
    w = weights_ref[...]
    total = w[:, 0:1] + w[:, 1:2]
    rows = hidden_ref.shape[0]
    quarter = got_ref.shape[1]
    size = got_ref.shape[0]
    got = got_ref[...]
    result = hidden_ref[...].astype(F32)
    ids = lax.broadcasted_iota(jnp.int32, (4 * rows, size), 1)
    for k in range(2):
        pick = jnp.where(ids == cols_ref[:, k : k + 1], 1.0, 0.0).astype(BF16)
        taken = jnp.dot(pick, got, preferred_element_type=F32)
        taken = jnp.concatenate([taken[q * rows : (q + 1) * rows] for q in range(4)], axis=1)
        result = result + (w[:, k : k + 1] / total) * taken
    out_ref[...] = result.astype(BF16)


def local(
    wide_inputs, narrow_inputs, wide_poles, narrow_poles, step_sizes, forget, wide_in_map,
    narrow_in_map, wide_out_map, narrow_out_map, skip_weight, gate_mix, residual, mixer_gain,
    out_proj, ffn_gain, routes, route_weights, gate_proj, up_proj, down_proj,
):
    me = lax.axis_index(SP).astype(jnp.int32).reshape(1)
    gate_rows = gate_mix.reshape(2, 256, 16)
    set_out, near_proj = mixer(
        me, wide_inputs, narrow_inputs, wide_poles, narrow_poles, step_sizes, forget, wide_in_map,
        narrow_in_map, wide_out_map, narrow_out_map, skip_weight, gate_rows, out_proj,
    )
    rows = residual.shape[0]
    width = residual.shape[1]
    core = lax.axis_index("tp").astype(jnp.int32)
    halves = set_out.reshape(2, rows, 512)
    mine = lax.dynamic_index_in_dim(halves, core, 0, keepdims=False)
    other = lax.dynamic_index_in_dim(halves, 1 - core, 0, keepdims=False)
    other = lax.ppermute(other, "tp", [(0, 1), (1, 0)])
    experts = lax.axis_size(SP) * lax.axis_size("tp")
    hidden1, send, cols = pl.pallas_call(
        project_kernel,
        out_shape=(
            jax.ShapeDtypeStruct((rows, width), BF16),
            jax.ShapeDtypeStruct((experts * 8, width // 4), BF16),
            jax.ShapeDtypeStruct((4 * rows, LANES), jnp.int32),
        ),
        in_specs=[SMEM] + [VMEM] * 7,
        out_specs=(VMEM, VMEM, VMEM),
        compiler_params=grant(12),
        cost_estimate=cost(2),
        name="project",
    )(
        core.reshape(1), mine, other, routes.T, mixer_gain.reshape(1, -1), ffn_gain.reshape(1, -1),
        residual, near_proj,
    )
    exchange = lambda x: lax.all_to_all(
        x.reshape(experts, 8, width // 4), SP_TP, split_axis=0, concat_axis=0, tiled=True
    ).reshape(-1, width // 4)
    done = pl.pallas_call(
        experts_kernel,
        out_shape=jax.ShapeDtypeStruct((experts * 8, width // 4), BF16),
        in_specs=[VMEM] * 3 + [HBM],
        out_specs=VMEM,
        scratch_shapes=[
            pltpu.VMEM((2 * experts, width), BF16),
            pltpu.VMEM((2 * experts, gate_proj.shape[2]), BF16),
            pltpu.VMEM(down_proj.shape[1:], BF16),
            pltpu.SemaphoreType.DMA,
        ],
        compiler_params=grant(20),
        cost_estimate=cost(9),
        name="experts",
    )(exchange(send), gate_proj[0], up_proj[0], *far((down_proj[0],)))
    return pl.pallas_call(
        combine_kernel,
        out_shape=jax.ShapeDtypeStruct((rows, width), BF16),
        in_specs=[VMEM] * 4,
        out_specs=VMEM,
        compiler_params=grant(12),
        cost_estimate=cost(2),
        name="combine",
    )(exchange(done), cols, route_weights, hidden1)


def solution(mesh):
    finer = Mesh(mesh.devices.reshape(4, 4, 4, mesh.shape["tp"]), SP_TP)
    return jax.shard_map(
        local,
        mesh=finer,
        in_specs=(
            P(SP, "tp"),
            P(SP, "tp"),
            P(None, None, "tp", None),
            P(None, None, "tp", None),
            P(None, None, "tp"),
            P(None, None, "tp", SP),
            P(None, None, "tp", None, None),
            P(None, None, "tp", None, None),
            P(None, None, "tp", None, None),
            P(None, None, "tp", None, None),
            P(None, "tp"),
            P(None, "tp", None, None),
            P(SP_TP, None),
            P(),
            P(),
            P(),
            P(SP_TP, None),
            P(SP_TP, None),
            P(SP_TP, None, None),
            P(SP_TP, None, None),
            P(SP_TP, None, None),
        ),
        out_specs=P(SP_TP, None),
        check_vma=False,
    )
```

```python
import functools

import jax
import jax.numpy as jnp
from jax import lax
from jax.experimental import pallas as pl
from jax.experimental.pallas import tpu as pltpu
from jax.sharding import Mesh
from jax.sharding import PartitionSpec as P

SP = ("sp_0", "sp_1", "sp_2")
SP_TP = ("sp_0", "sp_1", "sp_2", "tp")
EPS = 1e-06
F32 = jnp.float32
BF16 = jnp.bfloat16
T = 128
LANES = 128
NT = (((1,), (1,)), ((), ()))
WIDE = (8, 2, 64)
NARROW = (4, 4, 32)


def started(sources, buffers, sems):
    copies = [
        pltpu.make_async_copy(source, buffer, sems.at[k])
        for k, (source, buffer) in enumerate(zip(sources, buffers))
    ]
    for copy in copies:
        copy.start()
    return copies


def lane_ids(shape):
    return lax.broadcasted_iota(jnp.int32, shape, len(shape) - 1)


def in_rows(grouped, kind):
    rows, parts, _ = kind
    return jnp.concatenate([grouped[rows * h : rows * (h + 1)] for h in range(parts)], axis=1)


def side_by_side(pieces, row, kind):
    rows, parts, _ = kind
    return jnp.concatenate([pieces[row + rows * h] for h in range(parts)], axis=1)


def padded8(rows):
    if rows.shape[0] == 8:
        return rows
    return jnp.concatenate([rows, jnp.zeros((8 - rows.shape[0], LANES), F32)], axis=0)


def discretized(poles_ref, d):
    pr, pi = poles_ref[d, 0], poles_ref[d, 1]
    growth = jnp.exp(pr)
    cr, ci = growth * jnp.cos(pi), growth * jnp.sin(pi)
    nr = cr - 1.0
    denom = pr * pr + pi * pi
    fr = (nr * pr + ci * pi) / denom
    fi = (ci * pr - nr * pi) / denom
    return cr, ci, fr, fi


def group_block(row, r, kind):
    rows, parts, states = kind
    ids = (lane_ids(row.shape) % LANES) // states
    zeros = lambda n: [jnp.zeros((n, 2 * LANES), BF16)] if n else []
    row = row.astype(F32)
    out, at = [], 0
    for h in range(parts):
        start = 16 * (r + rows * h)
        out += zeros(start - at) + [jnp.where(ids == h, row, 0.0).astype(BF16)]
        at = start + 16
    return jnp.concatenate(out + zeros(16 * 16 - at), axis=0)


def spread(table, base, r, kind):
    rows, parts, states = kind
    n = table.shape[0]
    lanes = lane_ids((n, LANES)) // states
    out = jnp.broadcast_to(table[:, base + r : base + r + 1], (n, LANES))
    for h in range(1, parts):
        k = base + r + rows * h
        out = jnp.where(lanes == h, jnp.broadcast_to(table[:, k : k + 1], (n, LANES)), out)
    return out


def push_into(steps_ref, which, d, u, poles_ref, in_ref, kind, re_ref, im_ref):
    rows, parts, _ = kind
    cr, ci, fr, fi = discretized(poles_ref, d)
    for r in range(rows):
        re, im = [], []
        for h in range(parts):
            g = r + rows * h
            step = steps_ref[d, which, g]
            gr, gi = fr[g : g + 1] * step, fi[g : g + 1] * step
            br, bi = in_ref[d, 0, g], in_ref[d, 1, g]
            re.append(gr * br - gi * bi)
            im.append(gr * bi + gi * br)
        row = jnp.concatenate([jnp.concatenate(re, axis=1), jnp.concatenate(im, axis=1)], axis=1)
        driven = jnp.dot(u, group_block(row, r, kind), preferred_element_type=F32)
        re_ref[pl.ds(r, T, stride=8), :] = driven[:, :LANES]
        im_ref[pl.ds(r, T, stride=8), :] = driven[:, LANES:]
    return padded8(in_rows(cr, kind)), padded8(in_rows(ci, kind))


def forget_columns(forget_ref):
    both = forget_ref[...]
    return jnp.transpose(jnp.concatenate([both, both], axis=0))


def load_pushes(copies, buffers, scr):
    wu_ref, nu_ref, wp_ref, np_ref, wi_ref, ni_ref, forget_ref, steps_ref = buffers
    copies[6].wait()
    forget_t = forget_columns(forget_ref)
    kept = jnp.exp(-forget_t)
    sets = ((WIDE, wu_ref, wp_ref, wi_ref), (NARROW, nu_ref, np_ref, ni_ref))
    for d in range(2):
        for which in range(2):
            k = d * 2 + which
            kind = sets[which][0]
            e_ref = scr[3 * k + 2]
            for r in range(kind[0]):
                e_ref[pl.ds(r, T, stride=8), :] = spread(kept, k * 16, r, kind)
    for k in (0, 1, 2, 3, 4, 5, 7):
        copies[k].wait()
    turns = []
    for d in range(2):
        for which, (kind, u_ref, poles_ref, in_ref) in enumerate(sets):
            k = d * 2 + which
            re_ref, im_ref, _ = scr[3 * k : 3 * k + 3]
            turns.append(
                push_into(steps_ref, which, d, u_ref[...], poles_ref, in_ref, kind, re_ref, im_ref)
            )
    return turns, forget_t


def three_terms(x):
    hi = x.astype(BF16).astype(F32)
    mid = (x - hi).astype(BF16).astype(F32)
    return hi, mid, x - hi - mid


def ends_kernel(me_ref, *refs):
    sources, send_ref, buffers, sems, scr = refs[:8], refs[8], refs[9:17], refs[17], refs[18:]
    turns, forget_t = load_pushes(started(sources, buffers, sems), buffers, scr)

    def step(t, state):
        new = []
        for k in range(4):
            re_ref, im_ref, e_ref = scr[3 * k : 3 * k + 3]
            at = pl.multiple_of((t if k < 2 else T - 1 - t) * 8, 8)
            (cr, ci), (sr, si) = turns[k], state[k]
            e = e_ref[pl.ds(at, 8), :]
            new.append(
                (
                    e * (cr * sr - ci * si) + re_ref[pl.ds(at, 8), :],
                    e * (cr * si + ci * sr) + im_ref[pl.ds(at, 8), :],
                )
            )
        return tuple(new)

    zero = jnp.zeros((8, LANES), F32)
    state = lax.fori_loop(0, T, step, ((zero, zero),) * 4, unroll=8)
    kept = jnp.exp(-jnp.sum(forget_t, axis=0, keepdims=True))
    hi, mid, lo = three_terms(kept)
    first = lane_ids((1, LANES)) < 64
    terms = jnp.where(first, hi, mid)
    rest = jnp.where(first, lo, 0.0)
    row = lax.broadcasted_iota(jnp.int32, (8, LANES), 0)
    blocks = []
    for d in range(2):
        (wr, wi), (nr, ni) = state[2 * d], state[2 * d + 1]
        nr = jnp.where(row < 4, nr, jnp.where(row == 4, terms, jnp.where(row == 5, rest, 0.0)))
        blocks.append(jnp.concatenate([wr, wi, nr, jnp.where(row < 4, ni, 0.0)], axis=0))
    me = me_ref[0]

    def put(j, _):
        at = pl.multiple_of(j * 32, 32)
        send_ref[pl.ds(at, 32), :] = jnp.where(j > me, blocks[0], blocks[1]).astype(BF16)
        return 0

    lax.fori_loop(0, send_ref.shape[0] // 32, put, 0)


def read_blocks(out_ref, d, r, kind):
    return side_by_side(out_ref[d, 0], r, kind), side_by_side(out_ref[d, 1], r, kind)


def local_kernel(*refs):
    sources, (y_ref, decay_ref, factor_ref), buffers = refs[:10], refs[11:14], refs[14:24]
    sems, scr = refs[24], refs[25:]
    copies = started(sources, buffers, sems)
    turns, _ = load_pushes(copies, buffers[:8], scr)
    wo_ref, no_ref = buffers[8:]
    prods = scr[12:]

    def step(t, state):
        new = []
        for k in range(4):
            re_ref, im_ref, e_ref = scr[3 * k : 3 * k + 3]
            at = pl.ds(pl.multiple_of((t if k < 2 else T - 1 - t) * 8, 8), 8)
            (cr, ci), (sr, si, pr, pi) = turns[k], state[k]
            e = e_ref[at, :]
            got = (
                e * (cr * sr - ci * si) + re_ref[at, :],
                e * (cr * si + ci * sr) + im_ref[at, :],
                e * (cr * pr - ci * pi),
                e * (cr * pi + ci * pr),
            )
            re_ref[at, :], im_ref[at, :] = got[0], got[1]
            prods[2 * k][at, :], prods[2 * k + 1][at, :] = got[2], got[3]
            new.append(got)
        return tuple(new)

    zero = jnp.zeros((8, LANES), F32)
    lax.fori_loop(0, T, step, ((zero, zero, zero + 1.0, zero),) * 4, unroll=4)
    copies[8].wait()
    copies[9].wait()
    for which, (kind, out_ref) in enumerate(((WIDE, wo_ref), (NARROW, no_ref))):
        total = jnp.zeros((T, 2 * LANES), F32)
        for d in range(2):
            k = d * 2 + which
            for r in range(kind[0]):
                at = pl.ds(r, T, stride=8)
                o_re, o_im = read_blocks(out_ref, d, r, kind)
                weights = group_block(jnp.concatenate([o_re, -o_im], axis=1), r, kind)
                hidden = jnp.concatenate([scr[3 * k][at, :], scr[3 * k + 1][at, :]], axis=1)
                total += lax.dot_general(
                    hidden.astype(BF16), weights, NT, preferred_element_type=F32
                )
                decay = jnp.concatenate([prods[2 * k][at, :], prods[2 * k + 1][at, :]], axis=1)
                first = ((d * 12) + which * 8 + r) * 2 * LANES
                decay_ref[:, first : first + 2 * LANES] = decay.astype(BF16)
        y_ref[:, which * 2 * LANES : (which + 1) * 2 * LANES] = total
    for k in range(4):
        cr, ci = turns[k]
        for _ in range(7):
            cr, ci = cr * cr - ci * ci, 2.0 * cr * ci
        factor_ref[16 * k : 16 * k + 8, :], factor_ref[16 * k + 8 : 16 * k + 16, :] = cr, ci


def carry_kernel(me_ref, got_ref, y_ref, decay_ref, factor_ref, *refs):
    sources, out_ref, weights_ref, buffers = refs[:7], refs[7], refs[8], refs[9:15]
    sems, flat, kept = refs[15], refs[16], refs[17:]
    copies = started(sources, buffers + (weights_ref,), sems)
    wu_ref, nu_ref, wo_ref, no_ref, skip_ref, gate_ref = buffers
    me = me_ref[0]
    blocks = got_ref.shape[0] // 32
    flat[...] = got_ref[...].astype(F32)
    first = flat[pl.ds(20, blocks, stride=32), :]
    table = first + pltpu.roll(first, 64, 1) + flat[pl.ds(21, blocks, stride=32), :]
    turns = []
    for d in range(2):
        for which, kind in enumerate((WIDE, NARROW)):
            k = d * 2 + which
            for r in range(kind[0]):
                kept[k][pl.ds(r, blocks, stride=8), :] = spread(table, k * 16, r, kind)
            turns.append(
                (factor_ref[16 * k : 16 * k + 8, :], factor_ref[16 * k + 8 : 16 * k + 16, :])
            )

    def step(i, state):
        new = []
        for k in range(4):
            j = i if k < 2 else blocks - 1 - i
            used = (j < me) if k < 2 else (j > me)
            base = pl.multiple_of(j * 32, 32)
            re_at, im_at = (0, 8) if k % 2 == 0 else (16, 24)
            (cr, ci), (sr, si) = turns[k], state[k]
            e = kept[k][pl.ds(pl.multiple_of(j * 8, 8), 8), :]
            re = e * (cr * sr - ci * si) + flat[pl.ds(base + re_at, 8), :]
            im = e * (cr * si + ci * sr) + flat[pl.ds(base + im_at, 8), :]
            new.append((jnp.where(used, re, sr), jnp.where(used, im, si)))
        return tuple(new)

    zero = jnp.zeros((8, LANES), F32)
    state = lax.fori_loop(0, blocks, step, ((zero, zero),) * 4, unroll=4)
    for copy in copies[:6]:
        copy.wait()
    for which, (kind, u_ref, o_ref) in enumerate(((WIDE, wu_ref, wo_ref), (NARROW, nu_ref, no_ref))):
        span = slice(which * 2 * LANES, (which + 1) * 2 * LANES)
        total = y_ref[:, span]
        for d in range(2):
            sr, si = state[d * 2 + which]
            for r in range(kind[0]):
                o_re, o_im = read_blocks(o_ref, d, r, kind)
                cr, ci = sr[r : r + 1], si[r : r + 1]
                row = jnp.concatenate([o_re * cr - o_im * ci, -(o_re * ci + o_im * cr)], axis=1)
                at = ((d * 12) + which * 8 + r) * 2 * LANES
                total += lax.dot_general(
                    decay_ref[:, at : at + 2 * LANES], group_block(row, r, kind), NT,
                    preferred_element_type=F32,
                )
        shaped = total + skip_ref[which : which + 1].astype(F32) * u_ref[...].astype(F32)
        inner = 0.7978845608028654 * (shaped + 0.044715 * (shaped * shaped * shaped))
        active = 0.5 * shaped * (1.0 + jnp.tanh(inner))
        hi = active.astype(BF16)
        lo = (active - hi.astype(F32)).astype(BF16)
        spread_out = jnp.where(
            lane_ids((16, 256)) % 16 == lax.broadcasted_iota(jnp.int32, (16, 256), 0), 1.0, 0.0
        ).astype(BF16)
        gate = jnp.dot(gate_ref[which], spread_out, preferred_element_type=F32)
        own = lax.broadcasted_iota(jnp.int32, (256, 256), 0) // 16 == lane_ids((256, 256)) // 16
        gate = jnp.where(own, gate, 0.0).astype(BF16)
        mixed = jnp.dot(hi, gate, preferred_element_type=F32) + jnp.dot(
            lo, gate, preferred_element_type=F32
        )
        out_ref[:, span] = (active * jax.nn.sigmoid(mixed)).astype(BF16)
    copies[6].wait()


SMEM = pl.BlockSpec(memory_space=pltpu.SMEM)
VMEM = pl.BlockSpec(memory_space=pltpu.VMEM)
HBM = pl.BlockSpec(memory_space=pltpu.HBM)
MIB = 2**20


def column(n):
    return pltpu.VMEM((8 * n, LANES), F32)


def fetched(arrays):
    return [
        (pltpu.SMEM if a.shape == (2, 2, 16) else pltpu.VMEM)(a.shape, a.dtype) for a in arrays
    ] + [pltpu.SemaphoreType.DMA((len(arrays),))]


def near(arrays):
    return tuple(pltpu.with_memory_space_constraint(a, pltpu.VMEM) for a in arrays)


def far(arrays):
    return tuple(pltpu.with_memory_space_constraint(a, pltpu.HBM) for a in arrays)


def cost(us):
    return pl.CostEstimate(flops=int(us * 1e9), bytes_accessed=int(us * 1e6), transcendentals=0)


def grant(mib):
    return pltpu.CompilerParams(vmem_limit_bytes=mib * MIB)


def mixer(me, wide_u, narrow_u, wide_p, narrow_p, steps, forget, wide_in, narrow_in, wide_out,
          narrow_out, skip, gate, out_proj):
    blocks = lax.axis_size(SP)
    forget = forget.reshape(-1, T)
    shared = far((wide_u, narrow_u, wide_p, narrow_p, wide_in, narrow_in, forget, steps))
    send = pl.pallas_call(
        ends_kernel,
        out_shape=jax.ShapeDtypeStruct((blocks * 32, LANES), BF16),
        in_specs=[SMEM] + [HBM] * 8,
        out_specs=VMEM,
        scratch_shapes=fetched(shared) + [column(T)] * 12,
        compiler_params=grant(20),
        cost_estimate=cost(6),
        name="ends",
    )(me, *shared)
    got = lax.all_to_all(
        send.reshape(blocks, 32, LANES), SP, split_axis=0, concat_axis=0, tiled=True
    )
    sources = shared + far((wide_out, narrow_out))
    y, decay, factors = pl.pallas_call(
        local_kernel,
        out_shape=(
            pltpu.VMEM((T, 4 * LANES), F32),
            pltpu.VMEM((T, 24 * 2 * LANES), BF16),
            pltpu.VMEM((64, LANES), F32),
        ),
        in_specs=[HBM] * 11,
        out_specs=(VMEM, VMEM, VMEM),
        scratch_shapes=fetched(sources) + [column(T)] * 20,
        compiler_params=grant(24),
        cost_estimate=cost(8),
        name="local",
    )(*sources, *far((send,)))
    sources = far(
        (wide_u, narrow_u, wide_out, narrow_out, skip, gate, out_proj)
    )
    return pl.pallas_call(
        carry_kernel,
        out_shape=(
            jax.ShapeDtypeStruct((T, 4 * LANES), BF16),
            jax.ShapeDtypeStruct(out_proj.shape, BF16),
        ),
        in_specs=[SMEM] + [VMEM] * 4 + [HBM] * 7,
        out_specs=(VMEM, VMEM),
        scratch_shapes=[pltpu.VMEM(a.shape, a.dtype) for a in sources[:6]]
        + [pltpu.SemaphoreType.DMA((7,))]
        + [pltpu.VMEM((blocks * 32, LANES), F32)] + [column(blocks)] * 4,
        compiler_params=grant(16),
        cost_estimate=cost(5),
        name="carry",
    )(me, got.reshape(-1, LANES), *near((y, decay, factors)), *sources)


def places(routes):
    n = routes.shape[1]
    flat = jnp.concatenate([routes, routes], axis=1).astype(F32)
    line = [flat[k : k + 1] for k in range(2)]
    first = lax.broadcasted_iota(jnp.int32, (2 * n, 2 * n), 0) == 0
    table = jnp.transpose(jnp.where(first, line[0], line[1]))
    lanes, rows = lane_ids((n, 2 * n)), lax.broadcasted_iota(jnp.int32, (n, 2 * n), 0)
    wide = [jnp.broadcast_to(table[:n, k : k + 1], (n, 2 * n)) for k in range(2)]
    across, down = [], []
    for k in range(2):
        over, under = 0.0, 0.0
        for o in range(2):
            over += jnp.where((rows < lanes % n) & (wide[o] == line[k]), 1.0, 0.0)
            under += jnp.where((lanes < rows) & (wide[k] == line[o]), 1.0, 0.0)
        at = line[k] * 8.0 + jnp.sum(over, axis=0, keepdims=True) + 2.0 * (lanes[:1] // n)
        across.append(jnp.concatenate([at, at + 4.0], axis=1).astype(jnp.int32))
        at = table[:n, k : k + 1] * 8.0 + jnp.sum(under, axis=1, keepdims=True)
        down.append(jnp.concatenate([at + 2.0 * q for q in range(4)], axis=0).astype(jnp.int32))
    return across, down


def project_kernel(
    core_ref, mine_ref, other_ref, routes_ref, gain_ref, ffn_ref, residual_ref, proj_ref,
    hidden_ref, send_ref, cols_ref,
):
    across, down = places(routes_ref[...])
    shape = cols_ref.shape
    cols_ref[...] = jnp.where(
        lane_ids(shape) == 0, jnp.broadcast_to(down[0], shape), jnp.broadcast_to(down[1], shape)
    )
    swap = core_ref[0] == 1
    mine, other = mine_ref[...].astype(F32), other_ref[...].astype(F32)
    first, second = jnp.where(swap, other, mine), jnp.where(swap, mine, other)
    half = first.shape[1] // 2
    joined = jnp.concatenate(
        [first[:, :half], second[:, :half], first[:, half:], second[:, half:]], axis=1
    )
    scale = lax.rsqrt(jnp.mean(joined * joined, axis=1, keepdims=True) + EPS)
    mixed = (joined * scale * gain_ref[...]).astype(BF16)
    projected = jnp.dot(mixed, proj_ref[...], preferred_element_type=F32)
    hidden1 = (residual_ref[...].astype(F32) + projected).astype(BF16)
    hidden_ref[...] = hidden1
    wide = hidden1.astype(F32)
    scale = lax.rsqrt(jnp.mean(wide * wide, axis=1, keepdims=True) + EPS)
    normed = (wide * scale * ffn_ref[...]).astype(BF16)
    quarter = normed.shape[1] // 4
    stacked = jnp.concatenate([normed[:, q * quarter : (q + 1) * quarter] for q in range(4)], axis=0)
    size = stacked.shape[0]
    for b in range(send_ref.shape[0] // size):
        ids = lax.broadcasted_iota(jnp.int32, (size, size), 0) + b * size
        hit = (ids == across[0]) | (ids == across[1])
        pick = jnp.where(hit, 1.0, 0.0).astype(BF16)
        send_ref[b * size : (b + 1) * size, :] = jnp.dot(
            pick, stacked, preferred_element_type=F32
        ).astype(BF16)


def turned(back):
    out = lax.broadcasted_iota(jnp.int32, (256, 256), 0)
    src = lax.broadcasted_iota(jnp.int32, (256, 256), 1)
    if back:
        out, src = src, out
    wanted = ((out % 64) // 2) * 8 + (out // 64) * 2 + out % 2
    return jnp.where(src == wanted, 1.0, 0.0).astype(BF16)


def experts_kernel(
    in_ref, gate_ref, up_ref, far_ref, out_ref, x_ref, h_ref, down_ref, sem
):
    copy = pltpu.make_async_copy(far_ref, down_ref, sem)
    copy.start()
    quarter = in_ref.shape[1]
    turn = turned(False)
    for b in range(4):
        got = jnp.dot(
            turn, in_ref[b * 256 : (b + 1) * 256, :], preferred_element_type=F32
        ).astype(BF16)
        for q in range(4):
            x_ref[b * 64 : (b + 1) * 64, q * quarter : (q + 1) * quarter] = got[
                q * 64 : (q + 1) * 64
            ]
    x = x_ref[...]
    gate = jnp.dot(x, gate_ref[...], preferred_element_type=F32)
    up = jnp.dot(x, up_ref[...], preferred_element_type=F32)
    h_ref[...] = (gate * jax.nn.sigmoid(gate) * up).astype(BF16)
    copy.wait()
    done = jnp.dot(h_ref[...], down_ref[...], preferred_element_type=F32).astype(BF16)
    back = turned(True)
    for b in range(4):
        stacked = jnp.concatenate(
            [
                done[b * 64 : (b + 1) * 64, q * quarter : (q + 1) * quarter] for q in range(4)
            ],
            axis=0,
        )
        out_ref[b * 256 : (b + 1) * 256, :] = jnp.dot(
            back, stacked, preferred_element_type=F32
        ).astype(BF16)


def combine_kernel(got_ref, cols_ref, weights_ref, hidden_ref, out_ref):
    w = weights_ref[...]
    total = w[:, 0:1] + w[:, 1:2]
    rows = hidden_ref.shape[0]
    quarter = got_ref.shape[1]
    size = got_ref.shape[0]
    got = got_ref[...]
    result = hidden_ref[...].astype(F32)
    ids = lax.broadcasted_iota(jnp.int32, (4 * rows, size), 1)
    pick = jnp.concatenate(
        [jnp.where(ids == cols_ref[:, k : k + 1], 1.0, 0.0).astype(BF16) for k in range(2)], axis=0
    )
    both = jnp.dot(pick, got, preferred_element_type=F32)
    for k in range(2):
        parts = [both[(4 * k + q) * rows : (4 * k + q + 1) * rows] for q in range(4)]
        result = result + (w[:, k : k + 1] / total) * jnp.concatenate(parts, axis=1)
    out_ref[...] = result.astype(BF16)


def local(
    wide_inputs, narrow_inputs, wide_poles, narrow_poles, step_sizes, forget, wide_in_map,
    narrow_in_map, wide_out_map, narrow_out_map, skip_weight, gate_mix, residual, mixer_gain,
    out_proj, ffn_gain, routes, route_weights, gate_proj, up_proj, down_proj,
):
    me = lax.axis_index(SP).astype(jnp.int32).reshape(1)
    gate_rows = gate_mix.reshape(2, 256, 16)
    set_out, near_proj = mixer(
        me, wide_inputs, narrow_inputs, wide_poles, narrow_poles, step_sizes, forget, wide_in_map,
        narrow_in_map, wide_out_map, narrow_out_map, skip_weight, gate_rows, out_proj,
    )
    rows = residual.shape[0]
    width = residual.shape[1]
    core = lax.axis_index("tp").astype(jnp.int32)
    halves = set_out.reshape(2, rows, 512)
    mine = lax.dynamic_index_in_dim(halves, core, 0, keepdims=False)
    other = lax.dynamic_index_in_dim(halves, 1 - core, 0, keepdims=False)
    other = lax.ppermute(other, "tp", [(0, 1), (1, 0)])
    experts = lax.axis_size(SP) * lax.axis_size("tp")
    hidden1, send, cols = pl.pallas_call(
        project_kernel,
        out_shape=(
            jax.ShapeDtypeStruct((rows, width), BF16),
            jax.ShapeDtypeStruct((experts * 8, width // 4), BF16),
            jax.ShapeDtypeStruct((4 * rows, LANES), jnp.int32),
        ),
        in_specs=[SMEM] + [VMEM] * 7,
        out_specs=(VMEM, VMEM, VMEM),
        compiler_params=grant(12),
        cost_estimate=cost(60),
        name="project",
    )(
        core.reshape(1), mine, other, routes.T, mixer_gain.reshape(1, -1), ffn_gain.reshape(1, -1),
        residual, near_proj,
    )
    exchange = lambda x: lax.all_to_all(
        x.reshape(experts, 8, width // 4), SP_TP, split_axis=0, concat_axis=0, tiled=True
    ).reshape(-1, width // 4)
    done = pl.pallas_call(
        experts_kernel,
        out_shape=jax.ShapeDtypeStruct((experts * 8, width // 4), BF16),
        in_specs=[VMEM] * 3 + [HBM],
        out_specs=VMEM,
        scratch_shapes=[
            pltpu.VMEM((2 * experts, width), BF16),
            pltpu.VMEM((2 * experts, gate_proj.shape[2]), BF16),
            pltpu.VMEM(down_proj.shape[1:], BF16),
            pltpu.SemaphoreType.DMA,
        ],
        compiler_params=grant(20),
        cost_estimate=cost(9),
        name="experts",
    )(exchange(send), gate_proj[0], up_proj[0], *far((down_proj[0],)))
    return pl.pallas_call(
        combine_kernel,
        out_shape=jax.ShapeDtypeStruct((rows, width), BF16),
        in_specs=[VMEM] * 4,
        out_specs=VMEM,
        compiler_params=grant(12),
        cost_estimate=cost(2),
        name="combine",
    )(exchange(done), cols, route_weights, hidden1)


def solution(mesh):
    finer = Mesh(mesh.devices.reshape(4, 4, 4, mesh.shape["tp"]), SP_TP)
    return jax.shard_map(
        local,
        mesh=finer,
        in_specs=(
            P(SP, "tp"),
            P(SP, "tp"),
            P(None, None, "tp", None),
            P(None, None, "tp", None),
            P(None, None, "tp"),
            P(None, None, "tp", SP),
            P(None, None, "tp", None, None),
            P(None, None, "tp", None, None),
            P(None, None, "tp", None, None),
            P(None, None, "tp", None, None),
            P(None, "tp"),
            P(None, "tp", None, None),
            P(SP_TP, None),
            P(),
            P(),
            P(),
            P(SP_TP, None),
            P(SP_TP, None),
            P(SP_TP, None, None),
            P(SP_TP, None, None),
            P(SP_TP, None, None),
        ),
        out_specs=P(SP_TP, None),
        check_vma=False,
    )
```

```python
import functools

import jax
import jax.numpy as jnp
from jax import lax
from jax.experimental import pallas as pl
from jax.experimental.pallas import tpu as pltpu
from jax.sharding import Mesh
from jax.sharding import PartitionSpec as P

SP = ("sp_0", "sp_1", "sp_2")
SP_TP = ("sp_0", "sp_1", "sp_2", "tp")
EPS = 1e-06
F32 = jnp.float32
BF16 = jnp.bfloat16
T = 128
LANES = 128
NT = (((1,), (1,)), ((), ()))
WIDE = (8, 2, 64)
NARROW = (4, 4, 32)


def started(sources, buffers, sems):
    copies = [
        pltpu.make_async_copy(source, buffer, sems.at[k])
        for k, (source, buffer) in enumerate(zip(sources, buffers))
    ]
    for copy in copies:
        copy.start()
    return copies


def lane_ids(shape):
    return lax.broadcasted_iota(jnp.int32, shape, len(shape) - 1)


def in_rows(grouped, kind):
    rows, parts, _ = kind
    return jnp.concatenate([grouped[rows * h : rows * (h + 1)] for h in range(parts)], axis=1)


def side_by_side(pieces, row, kind):
    rows, parts, _ = kind
    return jnp.concatenate([pieces[row + rows * h] for h in range(parts)], axis=1)


def padded8(rows):
    if rows.shape[0] == 8:
        return rows
    return jnp.concatenate([rows, jnp.zeros((8 - rows.shape[0], LANES), F32)], axis=0)


def discretized(poles_ref, d):
    pr, pi = poles_ref[d, 0], poles_ref[d, 1]
    growth = jnp.exp(pr)
    cr, ci = growth * jnp.cos(pi), growth * jnp.sin(pi)
    nr = cr - 1.0
    denom = pr * pr + pi * pi
    fr = (nr * pr + ci * pi) / denom
    fi = (ci * pr - nr * pi) / denom
    return cr, ci, fr, fi


def group_block(row, r, kind):
    rows, parts, states = kind
    ids = (lane_ids(row.shape) % LANES) // states
    zeros = lambda n: [jnp.zeros((n, 2 * LANES), BF16)] if n else []
    row = row.astype(F32)
    out, at = [], 0
    for h in range(parts):
        start = 16 * (r + rows * h)
        out += zeros(start - at) + [jnp.where(ids == h, row, 0.0).astype(BF16)]
        at = start + 16
    return jnp.concatenate(out + zeros(16 * 16 - at), axis=0)


def spread(table, base, r, kind):
    rows, parts, states = kind
    n = table.shape[0]
    lanes = lane_ids((n, LANES)) // states
    out = jnp.broadcast_to(table[:, base + r : base + r + 1], (n, LANES))
    for h in range(1, parts):
        k = base + r + rows * h
        out = jnp.where(lanes == h, jnp.broadcast_to(table[:, k : k + 1], (n, LANES)), out)
    return out


def push_into(steps_ref, which, d, u, poles_ref, in_ref, kind, re_ref, im_ref):
    rows, parts, _ = kind
    cr, ci, fr, fi = discretized(poles_ref, d)
    for r in range(rows):
        re, im = [], []
        for h in range(parts):
            g = r + rows * h
            step = steps_ref[d, which, g]
            gr, gi = fr[g : g + 1] * step, fi[g : g + 1] * step
            br, bi = in_ref[d, 0, g], in_ref[d, 1, g]
            re.append(gr * br - gi * bi)
            im.append(gr * bi + gi * br)
        row = jnp.concatenate([jnp.concatenate(re, axis=1), jnp.concatenate(im, axis=1)], axis=1)
        driven = jnp.dot(u, group_block(row, r, kind), preferred_element_type=F32)
        re_ref[pl.ds(r, T, stride=8), :] = driven[:, :LANES]
        im_ref[pl.ds(r, T, stride=8), :] = driven[:, LANES:]
    return padded8(in_rows(cr, kind)), padded8(in_rows(ci, kind))


def forget_columns(forget_ref):
    both = forget_ref[...]
    return jnp.transpose(jnp.concatenate([both, both], axis=0))


def load_pushes(copies, buffers, scr):
    wu_ref, nu_ref, wp_ref, np_ref, wi_ref, ni_ref, forget_ref, steps_ref = buffers
    copies[6].wait()
    forget_t = forget_columns(forget_ref)
    kept = jnp.exp(-forget_t)
    sets = ((WIDE, wu_ref, wp_ref, wi_ref), (NARROW, nu_ref, np_ref, ni_ref))
    for d in range(2):
        for which in range(2):
            k = d * 2 + which
            kind = sets[which][0]
            e_ref = scr[3 * k + 2]
            for r in range(kind[0]):
                e_ref[pl.ds(r, T, stride=8), :] = spread(kept, k * 16, r, kind)
    for k in (0, 1, 2, 3, 4, 5, 7):
        copies[k].wait()
    turns = []
    for d in range(2):
        for which, (kind, u_ref, poles_ref, in_ref) in enumerate(sets):
            k = d * 2 + which
            re_ref, im_ref, _ = scr[3 * k : 3 * k + 3]
            turns.append(
                push_into(steps_ref, which, d, u_ref[...], poles_ref, in_ref, kind, re_ref, im_ref)
            )
    return turns, forget_t


def three_terms(x):
    hi = x.astype(BF16).astype(F32)
    mid = (x - hi).astype(BF16).astype(F32)
    return hi, mid, x - hi - mid


def ends_kernel(me_ref, *refs):
    sources, send_ref, buffers, sems, scr = refs[:8], refs[8], refs[9:17], refs[17], refs[18:30]
    blocks_ref = refs[30]
    turns, forget_t = load_pushes(started(sources, buffers, sems), buffers, scr)

    def step(t, state):
        new = []
        for k in range(4):
            re_ref, im_ref, e_ref = scr[3 * k : 3 * k + 3]
            at = pl.multiple_of((t if k < 2 else T - 1 - t) * 8, 8)
            (cr, ci), (sr, si) = turns[k], state[k]
            e = e_ref[pl.ds(at, 8), :]
            new.append(
                (
                    e * (cr * sr - ci * si) + re_ref[pl.ds(at, 8), :],
                    e * (cr * si + ci * sr) + im_ref[pl.ds(at, 8), :],
                )
            )
        return tuple(new)

    zero = jnp.zeros((8, LANES), F32)
    state = lax.fori_loop(0, T, step, ((zero, zero),) * 4, unroll=8)
    kept = jnp.exp(-jnp.sum(forget_t, axis=0, keepdims=True))
    hi, mid, lo = three_terms(kept)
    first = lane_ids((1, LANES)) < 64
    terms = jnp.where(first, hi, mid)
    rest = jnp.where(first, lo, 0.0)
    row = lax.broadcasted_iota(jnp.int32, (8, LANES), 0)
    blocks = []
    for d in range(2):
        (wr, wi), (nr, ni) = state[2 * d], state[2 * d + 1]
        nr = jnp.where(row < 4, nr, jnp.where(row == 4, terms, jnp.where(row == 5, rest, 0.0)))
        blocks.append(jnp.concatenate([wr, wi, nr, jnp.where(row < 4, ni, 0.0)], axis=0))
    me = me_ref[0]
    blocks_ref[...] = jnp.concatenate(blocks, axis=0).astype(BF16)

    def put(j, _):
        at = pl.multiple_of(j * 32, 32)
        start = pl.multiple_of(jnp.where(j > me, 0, 32), 32)
        send_ref[pl.ds(at, 32), :] = blocks_ref[pl.ds(start, 32), :]
        return 0

    lax.fori_loop(0, send_ref.shape[0] // 32, put, 0, unroll=8)


def read_blocks(out_ref, d, r, kind):
    return side_by_side(out_ref[d, 0], r, kind), side_by_side(out_ref[d, 1], r, kind)


def local_kernel(*refs):
    sources, (y_ref, decay_ref, factor_ref), buffers = refs[:10], refs[11:14], refs[14:24]
    sems, scr = refs[24], refs[25:]
    copies = started(sources, buffers, sems)
    turns, _ = load_pushes(copies, buffers[:8], scr)
    wo_ref, no_ref = buffers[8:]
    prods = scr[12:]

    def step(t, state):
        new = []
        for k in range(4):
            re_ref, im_ref, e_ref = scr[3 * k : 3 * k + 3]
            at = pl.ds(pl.multiple_of((t if k < 2 else T - 1 - t) * 8, 8), 8)
            (cr, ci), (sr, si, pr, pi) = turns[k], state[k]
            e = e_ref[at, :]
            got = (
                e * (cr * sr - ci * si) + re_ref[at, :],
                e * (cr * si + ci * sr) + im_ref[at, :],
                e * (cr * pr - ci * pi),
                e * (cr * pi + ci * pr),
            )
            re_ref[at, :], im_ref[at, :] = got[0], got[1]
            prods[2 * k][at, :], prods[2 * k + 1][at, :] = got[2], got[3]
            new.append(got)
        return tuple(new)

    zero = jnp.zeros((8, LANES), F32)
    lax.fori_loop(0, T, step, ((zero, zero, zero + 1.0, zero),) * 4, unroll=4)
    copies[8].wait()
    copies[9].wait()
    for which, (kind, out_ref) in enumerate(((WIDE, wo_ref), (NARROW, no_ref))):
        total = jnp.zeros((T, 2 * LANES), F32)
        for d in range(2):
            k = d * 2 + which
            for r in range(kind[0]):
                at = pl.ds(r, T, stride=8)
                o_re, o_im = read_blocks(out_ref, d, r, kind)
                weights = group_block(jnp.concatenate([o_re, -o_im], axis=1), r, kind)
                hidden = jnp.concatenate([scr[3 * k][at, :], scr[3 * k + 1][at, :]], axis=1)
                total += lax.dot_general(
                    hidden.astype(BF16), weights, NT, preferred_element_type=F32
                )
                decay = jnp.concatenate([prods[2 * k][at, :], prods[2 * k + 1][at, :]], axis=1)
                first = ((d * 12) + which * 8 + r) * 2 * LANES
                decay_ref[:, first : first + 2 * LANES] = decay.astype(BF16)
        y_ref[:, which * 2 * LANES : (which + 1) * 2 * LANES] = total
    for k in range(4):
        cr, ci = turns[k]
        for _ in range(7):
            cr, ci = cr * cr - ci * ci, 2.0 * cr * ci
        factor_ref[16 * k : 16 * k + 8, :], factor_ref[16 * k + 8 : 16 * k + 16, :] = cr, ci


def carry_kernel(me_ref, got_ref, y_ref, decay_ref, factor_ref, *refs):
    sources, out_ref, weights_ref, buffers = refs[:7], refs[7], refs[8], refs[9:15]
    sems, flat, kept = refs[15], refs[16], refs[17:]
    copies = started(sources, buffers + (weights_ref,), sems)
    wu_ref, nu_ref, wo_ref, no_ref, skip_ref, gate_ref = buffers
    me = me_ref[0]
    blocks = got_ref.shape[0] // 32
    flat[...] = got_ref[...].astype(F32)
    first = flat[pl.ds(20, blocks, stride=32), :]
    table = first + pltpu.roll(first, 64, 1) + flat[pl.ds(21, blocks, stride=32), :]
    turns = []
    for d in range(2):
        for which, kind in enumerate((WIDE, NARROW)):
            k = d * 2 + which
            for r in range(kind[0]):
                kept[k][pl.ds(r, blocks, stride=8), :] = spread(table, k * 16, r, kind)
            turns.append(
                (factor_ref[16 * k : 16 * k + 8, :], factor_ref[16 * k + 8 : 16 * k + 16, :])
            )

    def step(i, state):
        new = []
        for k in range(4):
            j = i if k < 2 else blocks - 1 - i
            used = (j < me) if k < 2 else (j > me)
            base = pl.multiple_of(j * 32, 32)
            re_at, im_at = (0, 8) if k % 2 == 0 else (16, 24)
            (cr, ci), (sr, si) = turns[k], state[k]
            e = kept[k][pl.ds(pl.multiple_of(j * 8, 8), 8), :]
            re = e * (cr * sr - ci * si) + flat[pl.ds(base + re_at, 8), :]
            im = e * (cr * si + ci * sr) + flat[pl.ds(base + im_at, 8), :]
            new.append((jnp.where(used, re, sr), jnp.where(used, im, si)))
        return tuple(new)

    zero = jnp.zeros((8, LANES), F32)
    state = lax.fori_loop(0, blocks, step, ((zero, zero),) * 4, unroll=4)
    for copy in copies[:6]:
        copy.wait()
    for which, (kind, u_ref, o_ref) in enumerate(((WIDE, wu_ref, wo_ref), (NARROW, nu_ref, no_ref))):
        span = slice(which * 2 * LANES, (which + 1) * 2 * LANES)
        total = y_ref[:, span]
        for d in range(2):
            sr, si = state[d * 2 + which]
            for r in range(kind[0]):
                o_re, o_im = read_blocks(o_ref, d, r, kind)
                cr, ci = sr[r : r + 1], si[r : r + 1]
                row = jnp.concatenate([o_re * cr - o_im * ci, -(o_re * ci + o_im * cr)], axis=1)
                at = ((d * 12) + which * 8 + r) * 2 * LANES
                total += lax.dot_general(
                    decay_ref[:, at : at + 2 * LANES], group_block(row, r, kind), NT,
                    preferred_element_type=F32,
                )
        shaped = total + skip_ref[which : which + 1].astype(F32) * u_ref[...].astype(F32)
        inner = 0.7978845608028654 * (shaped + 0.044715 * (shaped * shaped * shaped))
        active = 0.5 * shaped * (1.0 + jnp.tanh(inner))
        hi = active.astype(BF16)
        lo = (active - hi.astype(F32)).astype(BF16)
        spread_out = jnp.where(
            lane_ids((16, 256)) % 16 == lax.broadcasted_iota(jnp.int32, (16, 256), 0), 1.0, 0.0
        ).astype(BF16)
        gate = jnp.dot(gate_ref[which], spread_out, preferred_element_type=F32)
        own = lax.broadcasted_iota(jnp.int32, (256, 256), 0) // 16 == lane_ids((256, 256)) // 16
        gate = jnp.where(own, gate, 0.0).astype(BF16)
        mixed = jnp.dot(hi, gate, preferred_element_type=F32) + jnp.dot(
            lo, gate, preferred_element_type=F32
        )
        out_ref[:, span] = (active * jax.nn.sigmoid(mixed)).astype(BF16)
    copies[6].wait()


SMEM = pl.BlockSpec(memory_space=pltpu.SMEM)
VMEM = pl.BlockSpec(memory_space=pltpu.VMEM)
HBM = pl.BlockSpec(memory_space=pltpu.HBM)
MIB = 2**20


def column(n):
    return pltpu.VMEM((8 * n, LANES), F32)


def fetched(arrays):
    return [
        (pltpu.SMEM if a.shape == (2, 2, 16) else pltpu.VMEM)(a.shape, a.dtype) for a in arrays
    ] + [pltpu.SemaphoreType.DMA((len(arrays),))]


def near(arrays):
    return tuple(pltpu.with_memory_space_constraint(a, pltpu.VMEM) for a in arrays)


def far(arrays):
    return tuple(pltpu.with_memory_space_constraint(a, pltpu.HBM) for a in arrays)


def cost(us):
    return pl.CostEstimate(flops=int(us * 1e9), bytes_accessed=int(us * 1e6), transcendentals=0)


def grant(mib):
    return pltpu.CompilerParams(vmem_limit_bytes=mib * MIB)


def mixer(me, wide_u, narrow_u, wide_p, narrow_p, steps, forget, wide_in, narrow_in, wide_out,
          narrow_out, skip, gate, out_proj):
    blocks = lax.axis_size(SP)
    forget = forget.reshape(-1, T)
    shared = far((wide_u, narrow_u, wide_p, narrow_p, wide_in, narrow_in, forget, steps))
    send = pl.pallas_call(
        ends_kernel,
        out_shape=jax.ShapeDtypeStruct((blocks * 32, LANES), BF16),
        in_specs=[SMEM] + [HBM] * 8,
        out_specs=VMEM,
        scratch_shapes=fetched(shared) + [column(T)] * 12 + [pltpu.VMEM((64, LANES), BF16)],
        compiler_params=grant(20),
        cost_estimate=cost(6),
        name="ends",
    )(me, *shared)
    got = lax.all_to_all(
        send.reshape(blocks, 32, LANES), SP, split_axis=0, concat_axis=0, tiled=True
    )
    sources = shared + far((wide_out, narrow_out))
    y, decay, factors = pl.pallas_call(
        local_kernel,
        out_shape=(
            pltpu.VMEM((T, 4 * LANES), F32),
            pltpu.VMEM((T, 24 * 2 * LANES), BF16),
            pltpu.VMEM((64, LANES), F32),
        ),
        in_specs=[HBM] * 11,
        out_specs=(VMEM, VMEM, VMEM),
        scratch_shapes=fetched(sources) + [column(T)] * 20,
        compiler_params=grant(24),
        cost_estimate=cost(8),
        name="local",
    )(*sources, *far((send,)))
    sources = far(
        (wide_u, narrow_u, wide_out, narrow_out, skip, gate, out_proj)
    )
    return pl.pallas_call(
        carry_kernel,
        out_shape=(
            jax.ShapeDtypeStruct((T, 4 * LANES), BF16),
            jax.ShapeDtypeStruct(out_proj.shape, BF16),
        ),
        in_specs=[SMEM] + [VMEM] * 4 + [HBM] * 7,
        out_specs=(VMEM, VMEM),
        scratch_shapes=[pltpu.VMEM(a.shape, a.dtype) for a in sources[:6]]
        + [pltpu.SemaphoreType.DMA((7,))]
        + [pltpu.VMEM((blocks * 32, LANES), F32)] + [column(blocks)] * 4,
        compiler_params=grant(16),
        cost_estimate=cost(5),
        name="carry",
    )(me, got.reshape(-1, LANES), *near((y, decay, factors)), *sources)


def places(routes):
    n = routes.shape[1]
    flat = jnp.concatenate([routes, routes], axis=1).astype(F32)
    line = [flat[k : k + 1] for k in range(2)]
    first = lax.broadcasted_iota(jnp.int32, (2 * n, 2 * n), 0) == 0
    table = jnp.transpose(jnp.where(first, line[0], line[1]))
    lanes, rows = lane_ids((n, 2 * n)), lax.broadcasted_iota(jnp.int32, (n, 2 * n), 0)
    wide = [jnp.broadcast_to(table[:n, k : k + 1], (n, 2 * n)) for k in range(2)]
    across, down = [], []
    for k in range(2):
        over, under = 0.0, 0.0
        for o in range(2):
            over += jnp.where((rows < lanes % n) & (wide[o] == line[k]), 1.0, 0.0)
            under += jnp.where((lanes < rows) & (wide[k] == line[o]), 1.0, 0.0)
        at = line[k] * 8.0 + jnp.sum(over, axis=0, keepdims=True) + 2.0 * (lanes[:1] // n)
        across.append(jnp.concatenate([at, at + 4.0], axis=1).astype(jnp.int32))
        at = table[:n, k : k + 1] * 8.0 + jnp.sum(under, axis=1, keepdims=True)
        down.append(jnp.concatenate([at + 2.0 * q for q in range(4)], axis=0).astype(jnp.int32))
    return across, down


def project_kernel(
    core_ref, mine_ref, other_ref, routes_ref, gain_ref, ffn_ref, residual_ref, proj_ref,
    hidden_ref, send_ref, cols_ref,
):
    across, down = places(routes_ref[...])
    shape = cols_ref.shape
    cols_ref[...] = jnp.where(
        lane_ids(shape) == 0, jnp.broadcast_to(down[0], shape), jnp.broadcast_to(down[1], shape)
    )
    swap = core_ref[0] == 1
    mine, other = mine_ref[...].astype(F32), other_ref[...].astype(F32)
    first, second = jnp.where(swap, other, mine), jnp.where(swap, mine, other)
    half = first.shape[1] // 2
    joined = jnp.concatenate(
        [first[:, :half], second[:, :half], first[:, half:], second[:, half:]], axis=1
    )
    scale = lax.rsqrt(jnp.mean(joined * joined, axis=1, keepdims=True) + EPS)
    mixed = (joined * scale * gain_ref[...]).astype(BF16)
    projected = jnp.dot(mixed, proj_ref[...], preferred_element_type=F32)
    hidden1 = (residual_ref[...].astype(F32) + projected).astype(BF16)
    hidden_ref[...] = hidden1
    wide = hidden1.astype(F32)
    scale = lax.rsqrt(jnp.mean(wide * wide, axis=1, keepdims=True) + EPS)
    normed = (wide * scale * ffn_ref[...]).astype(BF16)
    quarter = normed.shape[1] // 4
    stacked = jnp.concatenate([normed[:, q * quarter : (q + 1) * quarter] for q in range(4)], axis=0)
    size = stacked.shape[0]
    for b in range(send_ref.shape[0] // size):
        ids = lax.broadcasted_iota(jnp.int32, (size, size), 0) + b * size
        hit = (ids == across[0]) | (ids == across[1])
        pick = jnp.where(hit, 1.0, 0.0).astype(BF16)
        send_ref[b * size : (b + 1) * size, :] = jnp.dot(
            pick, stacked, preferred_element_type=F32
        ).astype(BF16)


def turned(back):
    out = lax.broadcasted_iota(jnp.int32, (256, 256), 0)
    src = lax.broadcasted_iota(jnp.int32, (256, 256), 1)
    if back:
        out, src = src, out
    wanted = ((out % 64) // 2) * 8 + (out // 64) * 2 + out % 2
    return jnp.where(src == wanted, 1.0, 0.0).astype(BF16)


def experts_kernel(
    in_ref, gate_ref, up_ref, down_ref, out_ref, x_ref, h_ref
):
    quarter = in_ref.shape[1]
    turn = turned(False)
    for b in range(4):
        got = jnp.dot(
            turn, in_ref[b * 256 : (b + 1) * 256, :], preferred_element_type=F32
        ).astype(BF16)
        for q in range(4):
            x_ref[b * 64 : (b + 1) * 64, q * quarter : (q + 1) * quarter] = got[
                q * 64 : (q + 1) * 64
            ]
    x = x_ref[...]
    gate = jnp.dot(x, gate_ref[...], preferred_element_type=F32)
    up = jnp.dot(x, up_ref[...], preferred_element_type=F32)
    h_ref[...] = (gate * jax.nn.sigmoid(gate) * up).astype(BF16)
    done = jnp.dot(h_ref[...], down_ref[...], preferred_element_type=F32).astype(BF16)
    back = turned(True)
    for b in range(4):
        stacked = jnp.concatenate(
            [
                done[b * 64 : (b + 1) * 64, q * quarter : (q + 1) * quarter] for q in range(4)
            ],
            axis=0,
        )
        out_ref[b * 256 : (b + 1) * 256, :] = jnp.dot(
            back, stacked, preferred_element_type=F32
        ).astype(BF16)


def combine_kernel(got_ref, cols_ref, weights_ref, hidden_ref, out_ref):
    w = weights_ref[...]
    total = w[:, 0:1] + w[:, 1:2]
    rows = hidden_ref.shape[0]
    quarter = got_ref.shape[1]
    size = got_ref.shape[0]
    got = got_ref[...]
    result = hidden_ref[...].astype(F32)
    ids = lax.broadcasted_iota(jnp.int32, (4 * rows, size), 1)
    pick = jnp.concatenate(
        [jnp.where(ids == cols_ref[:, k : k + 1], 1.0, 0.0).astype(BF16) for k in range(2)], axis=0
    )
    both = jnp.dot(pick, got, preferred_element_type=F32)
    for k in range(2):
        parts = [both[(4 * k + q) * rows : (4 * k + q + 1) * rows] for q in range(4)]
        result = result + (w[:, k : k + 1] / total) * jnp.concatenate(parts, axis=1)
    out_ref[...] = result.astype(BF16)


def local(
    wide_inputs, narrow_inputs, wide_poles, narrow_poles, step_sizes, forget, wide_in_map,
    narrow_in_map, wide_out_map, narrow_out_map, skip_weight, gate_mix, residual, mixer_gain,
    out_proj, ffn_gain, routes, route_weights, gate_proj, up_proj, down_proj,
):
    me = lax.axis_index(SP).astype(jnp.int32).reshape(1)
    gate_rows = gate_mix.reshape(2, 256, 16)
    set_out, near_proj = mixer(
        me, wide_inputs, narrow_inputs, wide_poles, narrow_poles, step_sizes, forget, wide_in_map,
        narrow_in_map, wide_out_map, narrow_out_map, skip_weight, gate_rows, out_proj,
    )
    rows = residual.shape[0]
    width = residual.shape[1]
    core = lax.axis_index("tp").astype(jnp.int32)
    halves = set_out.reshape(2, rows, 512)
    mine = lax.dynamic_index_in_dim(halves, core, 0, keepdims=False)
    other = lax.dynamic_index_in_dim(halves, 1 - core, 0, keepdims=False)
    other = lax.ppermute(other, "tp", [(0, 1), (1, 0)])
    experts = lax.axis_size(SP) * lax.axis_size("tp")
    hidden1, send, cols = pl.pallas_call(
        project_kernel,
        out_shape=(
            jax.ShapeDtypeStruct((rows, width), BF16),
            jax.ShapeDtypeStruct((experts * 8, width // 4), BF16),
            jax.ShapeDtypeStruct((4 * rows, LANES), jnp.int32),
        ),
        in_specs=[SMEM] + [VMEM] * 7,
        out_specs=(VMEM, VMEM, VMEM),
        compiler_params=grant(12),
        cost_estimate=cost(60),
        name="project",
    )(
        core.reshape(1), mine, other, routes.T, mixer_gain.reshape(1, -1), ffn_gain.reshape(1, -1),
        residual, near_proj,
    )
    exchange = lambda x: lax.all_to_all(
        x.reshape(experts, 8, width // 4), SP_TP, split_axis=0, concat_axis=0, tiled=True
    ).reshape(-1, width // 4)
    done = pl.pallas_call(
        experts_kernel,
        out_shape=jax.ShapeDtypeStruct((experts * 8, width // 4), BF16),
        in_specs=[VMEM] * 4,
        out_specs=VMEM,
        scratch_shapes=[
            pltpu.VMEM((2 * experts, width), BF16),
            pltpu.VMEM((2 * experts, gate_proj.shape[2]), BF16),
        ],
        compiler_params=grant(12),
        cost_estimate=cost(9),
        name="experts",
    )(exchange(send), gate_proj[0], up_proj[0], down_proj[0])
    return pl.pallas_call(
        combine_kernel,
        out_shape=jax.ShapeDtypeStruct((rows, width), BF16),
        in_specs=[VMEM] * 4,
        out_specs=VMEM,
        compiler_params=grant(12),
        cost_estimate=cost(2),
        name="combine",
    )(exchange(done), cols, route_weights, hidden1)


def solution(mesh):
    finer = Mesh(mesh.devices.reshape(4, 4, 4, mesh.shape["tp"]), SP_TP)
    return jax.shard_map(
        local,
        mesh=finer,
        in_specs=(
            P(SP, "tp"),
            P(SP, "tp"),
            P(None, None, "tp", None),
            P(None, None, "tp", None),
            P(None, None, "tp"),
            P(None, None, "tp", SP),
            P(None, None, "tp", None, None),
            P(None, None, "tp", None, None),
            P(None, None, "tp", None, None),
            P(None, None, "tp", None, None),
            P(None, "tp"),
            P(None, "tp", None, None),
            P(SP_TP, None),
            P(),
            P(),
            P(),
            P(SP_TP, None),
            P(SP_TP, None),
            P(SP_TP, None, None),
            P(SP_TP, None, None),
            P(SP_TP, None, None),
        ),
        out_specs=P(SP_TP, None),
        check_vma=False,
    )
```
